32 devices in a mesh: ep: 4 (over y, x), tp: 8 (over z, core).
Axes of the slice: x: 2, y: 2, z: 4, core: 2. Of those that a mesh axis runs over, the one named last changes fastest.
Arguments:
- tokens: bfloat16 [1024, 4096], P('ep'), may hold values from -6 to 6
- cotangent: bfloat16 [1024, 4096], P('ep'), may hold values from -6 to 6
- routing: int32 [1024, 2], P('ep'), may hold values from 0 to 3, all different within a row; in each aligned block of 256 rows (0 to 255, 256 to 511, ...) at most 160 rows name the same one
- group_gate: float32 [1024], P('ep'), may hold values from 0.2 to 1
- inner_gate: float32 [1024, 2], P('ep'), may hold values from 0.1 to 0.9
- w_gate: bfloat16 [4, 4096, 2048], P('ep', None, 'tp'), may hold values from -0.09375 to 0.09375
- w_up: bfloat16 [4, 4096, 2048], P('ep', None, 'tp'), may hold values from -0.09375 to 0.09375
- w_down: bfloat16 [4, 2048, 4096], P('ep', 'tp'), may hold values from -0.125 to 0.125
Outputs:
- token_grad: bfloat16 [1024, 4096], P('ep', 'tp')
- group_grad: float32 [1024], P('ep')
- inner_grad: float32 [1024, 2], P('ep')
- gate_weight_grad: bfloat16 [4, 4096, 2048], P('ep', None, 'tp')
- up_weight_grad: bfloat16 [4, 4096, 2048], P('ep', None, 'tp')
- down_weight_grad: bfloat16 [4, 2048, 4096], P('ep', 'tp')
The draws below stay inside these ranges and needn't reach their ends.
Inputs may be any that keep to these rules, and one draw needn't show every extreme that they name: `routing`: each row names 2 different experts. Among the rows of one device (aligned blocks of 256 rows) no expert is named more than 160 times, and in every draw some expert is named exactly 160 times in some block.
All inputs are finite; a program needn't handle non-finite values.
Results may differ from the reference program's by a relative error of at most 0.02.
Values may be sent and summed in bfloat16 or wider, within the bound.
A program may use at most 128 MiB of HBM per device.

```python
import math
import jax
import jax.numpy as jnp
import numpy as np
from jax import lax

D = 4096
FF = 2048
TOP = 2
TOK_DEV = 256
EXPERTS = 4
CAP = 160
TOKENS = 1024
N_EP = 4
N_TP = 8


def block_levels(rng, dims, split, least, high):
    factor_of, own = 1.0, jax.random.fold_in(rng, 6)
    for dim, blocks in split:
        draws = jnp.exp(jax.random.uniform(jax.random.fold_in(own, dim), (blocks,), jnp.float32, least / len(split), high / len(split)))
        factor_of = factor_of * jnp.repeat(draws, dims[dim] // blocks).reshape([-1 if axis == dim else 1 for axis in range(len(dims))])
    return factor_of


def deal_out(stream_key, own, number, rows, number_of, top, bound, lean):
    order = jax.random.permutation(stream_key, number_of)
    crowded, usual = load_shares(number_of, rows * top, bound, lean, True), load_shares(number_of, rows * top, bound, lean, False)
    places = jnp.arange(number_of)

    def named(tallies, turn):
        used = int((tallies > 0).sum())
        fixed = max(1, used // 4)
        passed = fixed + (places - fixed + turn * (used - fixed)) % max(1, number_of - fixed)
        return jnp.zeros((number_of,), jnp.int32).at[order[jnp.where(places < fixed, places, passed)]].set(jnp.asarray(tallies, jnp.int32))

    tallies = jnp.where(number % 4 == 0, named(crowded, number // 4), named(usual, number - number // 4 - 1))
    mixed = jax.random.permutation(jax.random.fold_in(own, 3), number_of)
    donor, taker = mixed[0:number_of // 2 * 2:2], mixed[1:number_of // 2 * 2:2]
    margin = jnp.minimum(tallies[donor] - 1, bound - tallies[taker]) // 2
    margin = jnp.where((donor == order[0]) | (taker == order[0]) | (tallies[taker] == 0), 0, jnp.maximum(margin, 0))
    passed = jax.random.randint(jax.random.fold_in(own, 4), (number_of // 2,), 0, 1 << 20) % (margin + 1)
    tallies = tallies.at[donor].add(-passed).at[taker].add(passed)
    members = jnp.searchsorted(jnp.cumsum(tallies), jnp.arange(rows * top), side="right").astype(jnp.int32)
    grid = members.reshape(top, rows).T
    grid = grid[jax.random.permutation(jax.random.fold_in(own, 1), rows)]
    turn = jax.random.randint(jax.random.fold_in(own, 2), (rows, 1), 0, top)
    return jnp.take_along_axis(grid, (jnp.arange(top)[None, :] + turn) % top, axis=1)


def load_shares(amount, total, bound, skew, full):
    portions = [(1 << 20) // math.isqrt(standing ** skew) + 1 for standing in range(1, amount + 1)]
    largest = bound if full else min(bound, max(-(-total // amount), total * portions[0] // sum(portions)))
    least = 1 if total - largest >= amount - 1 else 0
    given, rest = [largest] + [least] * (amount - 1), total - largest - least * (amount - 1)
    while rest > 0:
        movable = [i for i in range(1, amount) if given[i] < largest] or [i for i in range(1, amount) if given[i] < bound]
        mass, budget = sum([portions[i] for i in movable]), rest
        for i in movable:
            more = min(bound - given[i], max(1, budget * portions[i] // mass), rest)
            given[i] = given[i] + more
            rest = rest - more
    return np.array(given)


def centred(own_key, shape, deviation, limit, split=(), kind=jnp.bfloat16):
    drawn = deviation * jax.random.normal(own_key, shape, jnp.float32)
    if split:
        drawn = drawn * block_levels(own_key, shape, split, -0.22, 0.18)
    return jnp.clip(drawn, -limit, limit).astype(kind)


def setup_inputs(seed: int = 0) -> dict:
    seeds = jax.random.split(jax.random.key(seed), 9)
    tokens = centred(seeds[0], (TOKENS, D), 1.0, 6.0, ((0, 4),))
    cotangent = centred(seeds[1], (TOKENS, D), 1.0, 6.0, ((0, 4),))
    routing_keys = jax.random.split(jax.random.fold_in(seeds[2], 1), TOKENS // TOK_DEV)
    routing_turns = jax.random.permutation(jax.random.fold_in(seeds[2], 3), TOKENS // TOK_DEV)
    routing = jax.vmap(lambda own, number: deal_out(jax.random.fold_in(seeds[2], 2), own, number, TOK_DEV, EXPERTS, TOP, CAP, 2))(routing_keys, routing_turns).reshape((TOKENS, TOP))
    group_gate = jnp.clip(0.2 + 0.8 * jax.random.uniform(seeds[3], (TOKENS,), jnp.float32) ** block_levels(seeds[3], (TOKENS,), ((0, 4),), -0.2, 0.2), 0.2, 1.0)
    inner_gate = jnp.clip(0.1 + 0.79999997 * jax.random.uniform(seeds[4], (TOKENS, TOP), jnp.float32) ** block_levels(seeds[4], (TOKENS, TOP), ((0, 4),), -0.2, 0.2), 0.1, 0.9)
    w_gate = centred(seeds[5], (EXPERTS, D, FF), D ** -0.5, 0.09375, ((0, 4), (2, 8)))
    w_up = centred(seeds[6], (EXPERTS, D, FF), D ** -0.5, 0.09375, ((0, 4), (2, 8)))
    w_down = centred(seeds[7], (EXPERTS, FF, D), FF ** -0.5, 0.125, ((0, 4), (1, 8)))
    return dict(tokens=tokens, cotangent=cotangent, routing=routing, group_gate=group_gate, inner_gate=inner_gate, w_gate=w_gate, w_up=w_up, w_down=w_down)


def expert_backward(packed):
    rows_in, cot_rows, row_weight, gate_weight, up_weight, down_weight = packed
    gate_pre = jnp.dot(rows_in, gate_weight, preferred_element_type=jnp.float32)
    up_pre = jnp.dot(rows_in, up_weight, preferred_element_type=jnp.float32)
    sigmoid_gate = jax.nn.sigmoid(gate_pre)
    silu_gate = gate_pre * sigmoid_gate
    hidden = (silu_gate * up_pre).astype(jnp.bfloat16)
    scaled_cot = (row_weight[:, None] * cot_rows.astype(jnp.float32)).astype(jnp.bfloat16)
    down_grad = jnp.dot(hidden.T, scaled_cot, preferred_element_type=jnp.float32).astype(jnp.bfloat16)
    grad_hidden = jnp.dot(cot_rows, down_weight.T, preferred_element_type=jnp.float32)
    scores = jnp.sum(grad_hidden * hidden.astype(jnp.float32), axis=1)
    weighted = row_weight[:, None] * grad_hidden
    grad_gate_in = (weighted * up_pre * sigmoid_gate * (1.0 + gate_pre * (1.0 - sigmoid_gate))).astype(jnp.bfloat16)
    grad_up_in = (weighted * silu_gate).astype(jnp.bfloat16)
    gate_grad = jnp.dot(rows_in.T, grad_gate_in, preferred_element_type=jnp.float32).astype(jnp.bfloat16)
    upper_grad = jnp.dot(rows_in.T, grad_up_in, preferred_element_type=jnp.float32).astype(jnp.bfloat16)
    row_count = rows_in.shape[0]
    model_width = rows_in.shape[1]
    block_units = FF // N_TP
    gate_blocks = grad_gate_in.astype(jnp.float32).reshape(row_count, N_TP, block_units)
    up_blocks = grad_up_in.astype(jnp.float32).reshape(row_count, N_TP, block_units)
    gate_w_blocks = gate_weight.astype(jnp.float32).reshape(model_width, N_TP, block_units)
    up_w_blocks = up_weight.astype(jnp.float32).reshape(model_width, N_TP, block_units)
    partial_rows = (jnp.einsum('rnf,dnf->nrd', gate_blocks, gate_w_blocks, precision=lax.Precision.HIGHEST)
                    + jnp.einsum('rnf,dnf->nrd', up_blocks, up_w_blocks, precision=lax.Precision.HIGHEST))
    rounded_parts = partial_rows.astype(jnp.bfloat16).astype(jnp.float32)
    row_grad = jnp.sum(rounded_parts, axis=0).astype(jnp.bfloat16)
    return gate_grad, upper_grad, down_grad, row_grad, scores


def reference(tokens, cotangent, routing, group_gate, inner_gate, w_gate, w_up, w_down):
    token_count, model_width = tokens.shape
    slots_expert = N_EP * CAP
    total_slots = EXPERTS * slots_expert
    flat_route = routing.reshape(N_EP, TOK_DEV * TOP)
    one_hot = (flat_route[:, :, None] == jnp.arange(EXPERTS, dtype=jnp.int32)[None, None, :]).astype(jnp.int32)
    within = jnp.sum(one_hot * (jnp.cumsum(one_hot, axis=1) - 1), axis=2)
    source = jnp.arange(N_EP, dtype=jnp.int32)[:, None]
    slot_of = (flat_route * slots_expert + source * CAP + within).reshape(-1).astype(jnp.int32)
    token_of = jnp.arange(token_count * TOP, dtype=jnp.int32) // TOP
    combine = (group_gate[:, None] * inner_gate).reshape(-1)
    rows_in = jnp.zeros((total_slots, model_width), jnp.bfloat16).at[slot_of].set(tokens[token_of])
    cot_rows = jnp.zeros((total_slots, model_width), jnp.bfloat16).at[slot_of].set(cotangent[token_of])
    row_weight = jnp.zeros((total_slots,), jnp.float32).at[slot_of].set(combine)
    results = lax.map(expert_backward, (rows_in.reshape(EXPERTS, slots_expert, model_width),
                                        cot_rows.reshape(EXPERTS, slots_expert, model_width),
                                        row_weight.reshape(EXPERTS, slots_expert), w_gate, w_up, w_down))
    gate_grad, upper_grad, down_grad, row_grad, scores = results
    picked = row_grad.reshape(total_slots, model_width)[slot_of].astype(jnp.float32)
    token_grad = jnp.sum(picked.reshape(token_count, TOP, model_width), axis=1).astype(jnp.bfloat16)
    score_of = scores.reshape(total_slots)[slot_of].reshape(token_count, TOP)
    inner_grad = group_gate[:, None] * score_of
    group_grad = jnp.sum(inner_gate * score_of, axis=1)
    return token_grad, group_grad, inner_grad, gate_grad, upper_grad, down_grad
```

```python
import functools

import jax
import jax.numpy as jnp
from jax import lax
from jax.experimental import pallas as pl
from jax.experimental.pallas import tpu as pltpu
from jax.sharding import PartitionSpec as P

LANES = 128
STEPS = 4
BF16 = jnp.bfloat16
F32 = jnp.float32


def peer_of(me, d, n):
    if n & (n - 1):
        return lax.rem(2 * n + d - me, n)
    out, bit = me, 1
    while bit < n:
        if d & bit:
            out = out + bit * (1 - 2 * lax.rem(me // bit, 2))
        bit *= 2
    return out


def barrier(partners):
    sem = pltpu.get_barrier_semaphore()
    for ep, tp in partners:
        pl.semaphore_signal(
            sem, inc=1, device_id=(ep, tp), device_id_type=pl.DeviceIdType.MESH
        )
    return lambda: pl.semaphore_wait(sem, len(partners))


def remote(src, dst, send, recv, ep, tp):
    return pltpu.make_async_remote_copy(
        src_ref=src,
        dst_ref=dst,
        send_sem=send,
        recv_sem=recv,
        device_id=(ep, tp),
        device_id_type=pl.DeviceIdType.MESH,
    )


def dot_nt(a, b):
    return lax.dot_general(a, b, (((1,), (1,)), ((), ())), preferred_element_type=F32)


def layer_kernel(n_ep, n_tp, cap, route, gates, inner, tok_hbm, cot_hbm, wg_hbm, wu_hbm, wd_hbm,
                 out, group_out, inner_out, gate_out, up_out, down_out,
                 toks, sends, rows_v, wg, wu, wd, tab, put, pick,
                 cs, c_in, square, sc_in, tot, tot_in,
                 acc_g, acc_u, acc_h, ggu, hid,
                 first, first_in, second, second_in, across_v, across_in, own_total, third, third_in,
                 local, drain, recv, sib_recv, c_s, c_r, sc_s, sc_r, tot_s, tot_r,
                 s1, r1, s2, r2, s3, r3, sa, ra):
    ep, tp = lax.axis_index("ep"), lax.axis_index("tp")
    core = lax.rem(tp, 2)
    z = tp // 2
    nz = n_tp // 2
    sibling = tp + 1 - 2 * core
    across = tp + 2 - 4 * lax.rem(z, 2)
    spot = lax.rem(z, 4)
    is_end = jnp.logical_or(spot == 0, spot == 3)
    is_inner = jnp.logical_not(is_end)
    upper = spot // 2
    inward = tp + 2 - 4 * upper
    outward = tp - 2 + 4 * upper
    tokens, model = toks.shape[1], toks.shape[2]
    top = route.shape[0]
    half = model // 2
    chunk = half // (2 * STEPS)
    base = core * half
    rows = n_ep * cap
    capp = cs.shape[2]
    units = wg.shape[1]
    width = out.shape[1]
    near = [d for d in range(1, n_ep) if not d & (d - 1)]
    far = [d for d in range(1, n_ep) if d & (d - 1)]
    everyone = [(peer_of(ep, d, n_ep), tp) for d in range(1, n_ep)]
    everyone += [(ep, lax.rem(tp + k, n_tp)) for k in range(1, n_tp)]

    def cols(start, size):
        return pl.ds(pl.multiple_of(start, LANES), size)

    loads = []
    for h in (core, 1 - core):
        for a, src in enumerate((tok_hbm, cot_hbm)):
            part = cols(h * half, half)
            loads.append(pltpu.make_async_copy(
                src.at[:, part], toks.at[a, :, part], local.at[len(loads)]
            ))
    for src, dst in ((wg_hbm, wg), (wu_hbm, wu), (wd_hbm, wd)):
        loads.append(pltpu.make_async_copy(src, dst, local.at[len(loads)]))
    for load in loads:
        load.start()
    entered = barrier(everyone)

    route_v = route[...]
    expert = lax.broadcasted_iota(jnp.int32, (-(-n_ep // 16) * 16, tokens), 0)
    names = jnp.zeros(expert.shape, F32)
    for k in range(top):
        names = names + jnp.where(route_v[k : k + 1] == expert, 1.0, 0.0)
    earlier = jnp.where(
        lax.broadcasted_iota(jnp.int32, (tokens, tokens), 0)
        < lax.broadcasted_iota(jnp.int32, (tokens, tokens), 1), 1.0, 0.0,
    ).astype(BF16)
    rank = jnp.dot(names.astype(BF16), earlier, preferred_element_type=F32)
    place_of = (expert * cap).astype(F32) + rank
    tab[...] = jnp.zeros_like(tab)
    slot_r = []
    for k in range(top):
        slot = jnp.sum(
            jnp.where(route_v[k : k + 1] == expert, place_of, 0.0), axis=0, keepdims=True
        )
        slot_r.append(slot)
        tab[k : k + 1, :] = slot
        tab[top + k : top + k + 1, :] = gates[...] * inner[k : k + 1, :]
    turned = tab[...].T
    slot_c = [turned[:, k : k + 1] for k in range(top)]
    comb_c = [turned[:, top + k : top + k + 1] for k in range(top)]

    def one_hot(index, slots):
        hit = index == slots[0]
        for slot in slots[1:]:
            hit = jnp.logical_or(hit, index == slot)
        return jnp.where(hit, 1.0, 0.0).astype(BF16)

    put[...] = one_hot(
        lax.broadcasted_iota(jnp.int32, (rows, tokens), 0).astype(F32), slot_r
    )
    own_put = one_hot(
        (lax.broadcasted_iota(jnp.int32, (cap, tokens), 0) + ep * cap).astype(F32), slot_r
    )

    def piece(a, p, k, side):
        return rows_v.at[a, p, :, cols(base + (k + STEPS * side) * chunk, chunk)]

    def direct(a, d, k, side, slot=0):
        p = peer_of(ep, d, n_ep)
        return remote(
            sends.at[a, p, :, cols((k + STEPS * side) * chunk, chunk)],
            piece(a, ep, k, side),
            drain.at[slot], recv.at[a, d - 1, k, side], p, tp,
        )

    def along(a, d, k, side, slot, target):
        p = peer_of(ep, d, n_ep)
        return remote(
            piece(a, p, k, side), piece(a, p, k, side),
            drain.at[slot], recv.at[a, d - 1, k, side], ep, target,
        )

    def to_sibling(a, d, k, side):
        p = peer_of(ep, d, n_ep)
        return remote(
            piece(a, p, k, side), piece(a, p, k, side),
            drain.at[4], sib_recv.at[a, d - 1, k, side], ep, sibling,
        )

    def place(k):
        for side in (1, 0):
            at = (k + STEPS * side) * chunk
            for a in range(2):
                placed = jnp.dot(
                    put[...], toks[a, :, cols(base + at, chunk)], preferred_element_type=F32
                ).astype(BF16).reshape(n_ep, cap, chunk)
                sends[a, :, :, cols(at, chunk)] = placed
                rows_v[a, ep, :, cols(base + at, chunk)] = sends[a, ep, :, cols(at, chunk)]

    def send_out(k):
        @pl.when(is_end)
        def _():
            for side in (1, 0):
                for a in range(2):
                    for d in near:
                        direct(a, d, k, side).start()

            @pl.when(k == STEPS - 1)
            def _():
                for a in range(2):
                    for d in far:
                        direct(a, d, k, 1 - upper, 1).start()

        @pl.when(is_inner)
        def _():
            for a in range(2):
                for d in far:
                    direct(a, d, k, upper).start()
            for a in range(2):
                for d in near:
                    direct(a, d, k, 0).start()

    loads[0].wait()
    loads[1].wait()
    place(0)
    entered()
    send_out(0)

    def place_step(k, carry):
        place(k)
        send_out(k)
        return carry

    lax.fori_loop(1, STEPS, place_step, 0)

    lane = lax.broadcasted_iota(jnp.int32, (tokens, capp), 1)
    lane_f = lane.astype(F32)
    for e in range(n_ep):
        weight = jnp.zeros((tokens, capp), F32)
        for k in range(top):
            hit = jnp.logical_and(lane_f == slot_c[k] - float(e * cap), lane < cap)
            weight = weight + jnp.where(hit, comb_c[k], 0.0)
        cs[e] = jnp.sum(weight, axis=0, keepdims=True)
    c_sends = []
    for d in range(1, n_ep):
        p = peer_of(ep, d, n_ep)
        copy = remote(cs.at[p], c_in.at[ep], c_s.at[d - 1], c_r.at[d - 1], p, tp)
        copy.start()
        c_sends.append(copy)
    c_in[ep] = cs[ep]
    pick[...] = one_hot(
        lax.broadcasted_iota(jnp.int32, (tokens, rows), 1).astype(F32), slot_c
    )
    square[...] = jnp.zeros_like(square)
    acc_g[...] = jnp.zeros_like(acc_g)
    acc_u[...] = jnp.zeros_like(acc_u)
    acc_h[...] = jnp.zeros_like(acc_h)
    loads[2].wait()
    loads[3].wait()
    other = (1 - core) * half
    for a in range(2):
        def own_step(j, carry, a=a):
            part = cols(other + j * (half // 4), half // 4)
            rows_v[a, ep, :, part] = jnp.dot(
                own_put, toks[a, :, part], preferred_element_type=F32
            ).astype(BF16)
            return carry

        lax.fori_loop(0, 4, own_step, 0)
    for load in loads[4:]:
        load.wait()

    def accumulate(h, k):
        parts = [cols(h * half + (k + STEPS * side) * chunk, chunk) for side in range(2)]

        def source(a, part):
            return rows_v[a, :, :, part].reshape(rows, chunk)

        for acc, w in ((acc_g, wg), (acc_u, wu)):
            acc[...] += jnp.dot(
                source(0, parts[0]), w[parts[0], :], preferred_element_type=F32
            ) + jnp.dot(source(0, parts[1]), w[parts[1], :], preferred_element_type=F32)
        acc_h[...] += dot_nt(source(1, parts[0]), wd[:, parts[0]]) + dot_nt(
            source(1, parts[1]), wd[:, parts[1]]
        )

    def arrive(k, carry):
        @pl.when(is_end)
        def _():
            for side in (1, 0):
                for a in range(2):
                    for d in near:
                        direct(a, d, k, side).wait_recv()
                        if side:
                            along(a, d, k, side, 2, inward).start()
                        to_sibling(a, d, k, side).start()
            for side in (upper, 1 - upper):
                for a in range(2):
                    for d in far:
                        direct(a, d, k, side).wait_recv()
                        to_sibling(a, d, k, side).start()

        @pl.when(is_inner)
        def _():
            for a in range(2):
                for d in far:
                    direct(a, d, k, upper).wait_recv()
                    along(a, d, k, upper, 2, inward).start()
                    along(a, d, k, upper, 3, outward).start()
                    to_sibling(a, d, k, upper).start()
            for a in range(2):
                for d in near:
                    direct(a, d, k, 0).wait_recv()
                    to_sibling(a, d, k, 0).start()
            for a in range(2):
                for d in far:
                    direct(a, d, k, 1 - upper).wait_recv()

                    @pl.when(k < STEPS - 1)
                    def _():
                        along(a, d, k, 1 - upper, 3, outward).start()

                    to_sibling(a, d, k, 1 - upper).start()
            for a in range(2):
                for d in near:
                    direct(a, d, k, 1).wait_recv()
                    to_sibling(a, d, k, 1).start()

        accumulate(core, k)
        for a in range(2):
            for side in range(2):
                for d in range(1, n_ep):
                    to_sibling(a, d, k, side).wait_recv()
        accumulate(1 - core, k)
        return carry

    lax.fori_loop(0, STEPS, arrive, 0)
    for copy in c_sends:
        copy.wait_recv()

    for p in range(n_ep):
        part = pl.ds(p * cap, cap)
        weight = jnp.broadcast_to(c_in[p], (LANES, capp)).T[:cap, :1]
        gate, up, grad = acc_g[part, :], acc_u[part, :], acc_h[part, :]
        sig = jax.nn.sigmoid(gate)
        silu = gate * sig
        hidden = silu * up
        score = jnp.sum(grad * hidden.astype(BF16).astype(F32), axis=1, keepdims=True)
        square[:cap, :] = jnp.broadcast_to(score, (cap, LANES))
        sc_in[tp, p] = square[...].T[:1, :]
        weighted = weight * grad
        hid[part, :] = (weight * hidden).astype(BF16)
        ggu[part, :units] = (weighted * up * sig * (1.0 + gate * (1.0 - sig))).astype(BF16)
        ggu[part, units:] = (weighted * silu).astype(BF16)

    def partial(share):
        part = pl.ds(pl.multiple_of(share * width, width), width)
        return dot_nt(ggu[:, :units], wg[part, :]) + dot_nt(ggu[:, units:], wu[part, :])

    masks = [1] + list(range(nz - 1, 1, -1)) + [0]
    order = [peer_of(z, m, nz) for m in masks]
    waits = []
    halves, moves = {}, {}

    def give_half(i):
        first[i] = partial(2 * order[i] + 1 - core).astype(BF16)
        halves[i] = remote(first.at[i], first_in.at[i], s1.at[i], r1.at[i], ep, sibling)
        halves[i].start()

    def spread(i):
        for d in range(1, n_ep):
            p = peer_of(ep, d, n_ep)
            copy = remote(
                second.at[i - 1, p], second_in.at[i - 1, ep],
                s2.at[i - 1, d - 1], r2.at[i - 1, d - 1], p, tp,
            )
            copy.start()
            moves[i, d] = copy

    crossing = remote(across_v, across_in, sa, ra, ep, across)

    def join(i):
        total = partial(2 * order[i] + core)
        halves[i].wait_recv()
        total = total + first_in[i].astype(F32)
        if i == 0:
            across_v[...] = total.astype(BF16)
            crossing.start()
        elif i < nz - 1:
            second[i - 1] = total.astype(BF16).reshape(second.shape[1:])
            spread(i)
        else:
            own_total[...] = total

    for i in range(nz):
        give_half(i)
        if i:
            join(i - 1)
    join(nz - 1)
    sc_sends = []
    for k in range(1, n_tp):
        copy = remote(
            sc_in.at[tp], sc_in.at[tp], sc_s.at[k - 1], sc_r.at[k - 1],
            ep, lax.rem(tp + k, n_tp),
        )
        copy.start()
        sc_sends.append(copy)

    def tile(t):
        return pl.ds(pl.multiple_of(t * width, width), width)

    def gate_up_step(t, carry):
        both = lax.dot_general(
            rows_v[0, :, :, tile(t)].reshape(rows, width), ggu[...],
            (((0,), (0,)), ((), ())), preferred_element_type=F32,
        ).astype(BF16)
        gate_out[tile(t), :] = both[:, :units]
        up_out[tile(t), :] = both[:, units:]
        return carry

    hidden_t = hid[...].T

    def down_step(t, carry):
        down_out[:, tile(t)] = jnp.dot(
            hidden_t, rows_v[1, :, :, tile(t)].reshape(rows, width),
            preferred_element_type=F32,
        ).astype(BF16)
        return carry

    def gather_tokens(i):
        for d in range(1, n_ep):
            moves[i, d].wait_recv()
        second_in[i - 1, ep] = second[i - 1, ep]
        return jnp.dot(
            pick[...], second_in[i - 1].reshape(rows, width), preferred_element_type=F32
        )

    last = []

    def pass_on(i):
        third[i - 1] = gather_tokens(i).astype(BF16)
        copy = remote(
            third.at[i - 1], third_in.at[i - 1], s3.at[i - 1], r3.at[i - 1],
            ep, 2 * order[i] + core,
        )
        copy.start()
        last.append(copy)

    lax.fori_loop(0, n_tp, gate_up_step, 0)
    pass_on(1)
    lax.fori_loop(0, n_tp // 2, down_step, 0)
    crossing.wait_recv()
    total = own_total[...] + across_in[...].astype(F32)
    second[nz - 2] = total.astype(BF16).reshape(second.shape[1:])
    spread(nz - 1)
    for i in range(2, nz - 1):
        pass_on(i)

    for copy in sc_sends:
        copy.wait_recv()
    summed = sc_in[0]
    for t in range(1, n_tp):
        summed = summed + sc_in[t]
    tot[...] = summed
    tot_sends = []
    for d in range(1, n_ep):
        p = peer_of(ep, d, n_ep)
        copy = remote(tot.at[p], tot_in.at[ep], tot_s.at[d - 1], tot_r.at[d - 1], p, tp)
        copy.start()
        tot_sends.append(copy)
    tot_in[ep] = tot[ep]
    lax.fori_loop(n_tp // 2, n_tp, down_step, 0)
    for copy in tot_sends:
        copy.wait_recv()
    score_r = [jnp.zeros((1, tokens), F32) for _ in range(top)]
    for e in range(n_ep):
        column = jnp.broadcast_to(tot_in[e], (LANES, capp)).T[:cap, :1]
        index = (lax.broadcasted_iota(jnp.int32, (cap, tokens), 0) + e * cap).astype(F32)
        for k in range(top):
            score_r[k] = score_r[k] + jnp.sum(
                jnp.where(index == tab[k : k + 1, :], column, 0.0), axis=0, keepdims=True
            )
    group = jnp.zeros((1, tokens), F32)
    for k in range(top):
        inner_out[k : k + 1, :] = gates[...] * score_r[k]
        group = group + inner[k : k + 1, :] * score_r[k]
    group_out[...] = group

    total = gather_tokens(nz - 1)
    for i, copy in enumerate(last):
        copy.wait_recv()
        total = total + third_in[i].astype(F32)
    out[...] = total.astype(BF16)

    def drained(ref, slot):
        remote(ref, ref, drain.at[slot], drain.at[slot], ep, sibling).wait_send()

    @pl.when(is_end)
    def _():
        drained(sends.at[:, : len(near)], 0)
        if far:
            drained(sends.at[:, : len(far), :, :chunk], 1)
        drained(rows_v.at[:, : len(near), :, : half // 2], 2)

    @pl.when(is_inner)
    def _():
        drained(sends.at[:, : n_ep - 1, :, : half // 2], 0)
        if far:
            drained(rows_v.at[:, : len(far), :, : half // 2], 2)
            drained(rows_v.at[:, : len(far), :, : half - chunk], 3)

    drained(rows_v.at[:, : n_ep - 1, :, :half], 4)
    for copy in c_sends + sc_sends + tot_sends + list(halves.values()) + list(moves.values()) + last:
        copy.wait_send()
    crossing.wait_send()


def layer(n_ep, n_tp, cap, route, gates, inner, tokens, cotangent, wg, wu, wd):
    vmem = pl.BlockSpec(memory_space=pltpu.VMEM)
    any_spec = pl.BlockSpec(memory_space=pl.ANY)
    nz = n_tp // 2
    count, model = tokens.shape
    rows, units = n_ep * cap, wg.shape[1]
    width, half = model // n_tp, model // 2
    capp = -(-cap // LANES) * LANES
    dma = pltpu.SemaphoreType.DMA
    return pl.pallas_call(
        functools.partial(layer_kernel, n_ep, n_tp, cap),
        out_shape=(
            jax.ShapeDtypeStruct((count, width), BF16),
            jax.ShapeDtypeStruct(gates.shape, F32),
            jax.ShapeDtypeStruct(inner.shape, F32),
            jax.ShapeDtypeStruct(wg.shape, BF16),
            jax.ShapeDtypeStruct(wu.shape, BF16),
            jax.ShapeDtypeStruct(wd.shape, BF16),
        ),
        in_specs=[vmem] * 3 + [any_spec] * 5,
        out_specs=(vmem,) * 6,
        scratch_shapes=[
            pltpu.VMEM((2, count, model), BF16),
            pltpu.VMEM((2, n_ep, cap, half), BF16),
            pltpu.VMEM((2, n_ep, cap, model), BF16),
            pltpu.VMEM(wg.shape, BF16),
            pltpu.VMEM(wu.shape, BF16),
            pltpu.VMEM(wd.shape, BF16),
            pltpu.VMEM((8, count), F32),
            pltpu.VMEM((rows, count), BF16),
            pltpu.VMEM((count, rows), BF16),
            pltpu.VMEM((n_ep, 1, capp), F32),
            pltpu.VMEM((n_ep, 1, capp), F32),
            pltpu.VMEM((capp, LANES), F32),
            pltpu.VMEM((n_tp, n_ep, 1, capp), F32),
            pltpu.VMEM((n_ep, 1, capp), F32),
            pltpu.VMEM((n_ep, 1, capp), F32),
            pltpu.VMEM((rows, units), F32),
            pltpu.VMEM((rows, units), F32),
            pltpu.VMEM((rows, units), F32),
            pltpu.VMEM((rows, 2 * units), BF16),
            pltpu.VMEM((rows, units), BF16),
            pltpu.VMEM((nz, rows, width), BF16),
            pltpu.VMEM((nz, rows, width), BF16),
            pltpu.VMEM((nz - 1, n_ep, cap, width), BF16),
            pltpu.VMEM((nz - 1, n_ep, cap, width), BF16),
            pltpu.VMEM((rows, width), BF16),
            pltpu.VMEM((rows, width), BF16),
            pltpu.VMEM((rows, width), F32),
            pltpu.VMEM((nz - 2, count, width), BF16),
            pltpu.VMEM((nz - 2, count, width), BF16),
            dma((7,)),
            dma((5,)),
            dma((2, n_ep - 1, STEPS, 2)),
            dma((2, n_ep - 1, STEPS, 2)),
            dma((n_ep - 1,)), dma((n_ep - 1,)),
            dma((n_tp - 1,)), dma((n_tp - 1,)),
            dma((n_ep - 1,)), dma((n_ep - 1,)),
            dma((nz,)), dma((nz,)),
            dma((nz - 1, n_ep - 1)), dma((nz - 1, n_ep - 1)),
            dma((nz - 2,)), dma((nz - 2,)),
            dma, dma,
        ],
        compiler_params=pltpu.CompilerParams(
            collective_id=0, has_side_effects=True, vmem_limit_bytes=54 * 1024 * 1024
        ),
    )(route, gates, inner, tokens, cotangent, wg, wu, wd)


def deliver_kernel(count, *refs):
    sems = refs[-1]
    copies = [
        pltpu.make_async_copy(refs[i], refs[count + i], sems.at[i]) for i in range(count)
    ]
    for copy in copies:
        copy.start()
    for copy in copies:
        copy.wait()


def deliver(*arrays):
    count = len(arrays)
    return pl.pallas_call(
        functools.partial(deliver_kernel, count),
        out_shape=tuple(jax.ShapeDtypeStruct(a.shape, a.dtype) for a in arrays),
        in_specs=[pl.BlockSpec(memory_space=pltpu.VMEM)] * count,
        out_specs=(pl.BlockSpec(memory_space=pl.ANY),) * count,
        scratch_shapes=[pltpu.SemaphoreType.DMA((count,))],
    )(*arrays)


def per_device(tokens, cotangent, routing, group_gate, inner_gate, w_gate, w_up, w_down):
    n_ep, n_tp = lax.axis_size("ep"), lax.axis_size("tp")
    cap = tokens.shape[0] * routing.shape[1] * 5 // (4 * n_ep)
    results = layer(
        n_ep, n_tp, cap, routing.T, group_gate[None], inner_gate.T,
        tokens, cotangent, w_gate[0], w_up[0], w_down[0],
    )
    token_grad, group_grad, inner_grad, gate_grad, upper_grad, down_grad = deliver(*results)
    return (
        token_grad,
        group_grad[0],
        inner_grad.T,
        gate_grad[None],
        upper_grad[None],
        down_grad[None],
    )


def solution(mesh):
    return jax.shard_map(
        per_device,
        mesh=mesh,
        in_specs=(
            P("ep", None),
            P("ep", None),
            P("ep", None),
            P("ep"),
            P("ep", None),
            P("ep", None, "tp"),
            P("ep", None, "tp"),
            P("ep", "tp", None),
        ),
        out_specs=(
            P("ep", "tp"),
            P("ep"),
            P("ep", None),
            P("ep", None, "tp"),
            P("ep", None, "tp"),
            P("ep", "tp", None),
        ),
        check_vma=False,
    )
```

```python
import functools

import jax
import jax.numpy as jnp
from jax import lax
from jax.experimental import pallas as pl
from jax.experimental.pallas import tpu as pltpu
from jax.sharding import PartitionSpec as P

LANES = 128
STEPS = 4
BF16 = jnp.bfloat16
F32 = jnp.float32


def peer_of(me, d, n):
    if n & (n - 1):
        return lax.rem(2 * n + d - me, n)
    out, bit = me, 1
    while bit < n:
        if d & bit:
            out = out + bit * (1 - 2 * lax.rem(me // bit, 2))
        bit *= 2
    return out


def barrier(partners):
    sem = pltpu.get_barrier_semaphore()
    for ep, tp in partners:
        pl.semaphore_signal(
            sem, inc=1, device_id=(ep, tp), device_id_type=pl.DeviceIdType.MESH
        )
    return lambda: pl.semaphore_wait(sem, len(partners))


def remote(src, dst, send, recv, ep, tp):
    return pltpu.make_async_remote_copy(
        src_ref=src,
        dst_ref=dst,
        send_sem=send,
        recv_sem=recv,
        device_id=(ep, tp),
        device_id_type=pl.DeviceIdType.MESH,
    )


def dot_nt(a, b):
    return lax.dot_general(a, b, (((1,), (1,)), ((), ())), preferred_element_type=F32)


def layer_kernel(n_ep, n_tp, cap, route, gates, inner, tok_hbm, cot_hbm, wg_hbm, wu_hbm, wd_hbm,
                 out, group_out, inner_out, gate_out, up_out, down_out,
                 toks, sends, rows_v, wg, wu, wd, tab, put, pick,
                 cs, c_in, square, sc_in, tot, tot_in,
                 acc_g, acc_u, acc_h, ggu, hid,
                 first, first_in, second, second_in, across_v, across_in, own_total,
                 third, third_in, held, final_in,
                 local, drain, recv, sib_recv, c_s, c_r, sc_s, sc_r, tot_s, tot_r,
                 s1, r1, s2, r2, s3, r3, s4, r4, sa, ra):
    ep, tp = lax.axis_index("ep"), lax.axis_index("tp")
    core = lax.rem(tp, 2)
    z = tp // 2
    nz = n_tp // 2
    sibling = tp + 1 - 2 * core
    across = tp + 2 - 4 * lax.rem(z, 2)
    spot = lax.rem(z, 4)
    is_end = jnp.logical_or(spot == 0, spot == 3)
    is_inner = jnp.logical_not(is_end)
    upper = spot // 2
    inward = tp + 2 - 4 * upper
    outward = tp - 2 + 4 * upper
    tokens, model = toks.shape[1], toks.shape[2]
    top = route.shape[0]
    half = model // 2
    chunk = half // (2 * STEPS)
    base = core * half
    rows = n_ep * cap
    capp = cs.shape[2]
    units = wg.shape[1]
    width = out.shape[1]
    near = [d for d in range(1, n_ep) if not d & (d - 1)]
    far = [d for d in range(1, n_ep) if d & (d - 1)]
    everyone = [(peer_of(ep, d, n_ep), tp) for d in range(1, n_ep)]
    everyone += [(ep, lax.rem(tp + k, n_tp)) for k in range(1, n_tp)]

    def cols(start, size):
        return pl.ds(pl.multiple_of(start, LANES), size)

    loads = []
    for h in (core, 1 - core):
        for a, src in enumerate((tok_hbm, cot_hbm)):
            part = cols(h * half, half)
            loads.append(pltpu.make_async_copy(
                src.at[:, part], toks.at[a, :, part], local.at[len(loads)]
            ))
    for src, dst in ((wg_hbm, wg), (wu_hbm, wu), (wd_hbm, wd)):
        loads.append(pltpu.make_async_copy(src, dst, local.at[len(loads)]))
    for load in loads:
        load.start()
    entered = barrier(everyone)

    route_v = route[...]
    expert = lax.broadcasted_iota(jnp.int32, (-(-n_ep // 16) * 16, tokens), 0)
    names = jnp.zeros(expert.shape, F32)
    for k in range(top):
        names = names + jnp.where(route_v[k : k + 1] == expert, 1.0, 0.0)
    earlier = jnp.where(
        lax.broadcasted_iota(jnp.int32, (tokens, tokens), 0)
        < lax.broadcasted_iota(jnp.int32, (tokens, tokens), 1), 1.0, 0.0,
    ).astype(BF16)
    rank = jnp.dot(names.astype(BF16), earlier, preferred_element_type=F32)
    place_of = (expert * cap).astype(F32) + rank
    tab[...] = jnp.zeros_like(tab)
    slot_r = []
    for k in range(top):
        slot = jnp.sum(
            jnp.where(route_v[k : k + 1] == expert, place_of, 0.0), axis=0, keepdims=True
        )
        slot_r.append(slot)
        tab[k : k + 1, :] = slot
        tab[top + k : top + k + 1, :] = gates[...] * inner[k : k + 1, :]
    turned = tab[...].T
    slot_c = [turned[:, k : k + 1] for k in range(top)]
    comb_c = [turned[:, top + k : top + k + 1] for k in range(top)]

    def one_hot(index, slots):
        hit = index == slots[0]
        for slot in slots[1:]:
            hit = jnp.logical_or(hit, index == slot)
        return jnp.where(hit, 1.0, 0.0).astype(BF16)

    put[...] = one_hot(
        lax.broadcasted_iota(jnp.int32, (rows, tokens), 0).astype(F32), slot_r
    )
    own_put = one_hot(
        (lax.broadcasted_iota(jnp.int32, (cap, tokens), 0) + ep * cap).astype(F32), slot_r
    )

    def piece(a, p, k, side):
        return rows_v.at[a, p, :, cols(base + (k + STEPS * side) * chunk, chunk)]

    def direct(a, d, k, side, slot=0):
        p = peer_of(ep, d, n_ep)
        return remote(
            sends.at[a, p, :, cols((k + STEPS * side) * chunk, chunk)],
            piece(a, ep, k, side),
            drain.at[slot], recv.at[a, d - 1, k, side], p, tp,
        )

    def along(a, d, k, side, slot, target):
        p = peer_of(ep, d, n_ep)
        return remote(
            piece(a, p, k, side), piece(a, p, k, side),
            drain.at[slot], recv.at[a, d - 1, k, side], ep, target,
        )

    def to_sibling(a, d, k, side):
        p = peer_of(ep, d, n_ep)
        return remote(
            piece(a, p, k, side), piece(a, p, k, side),
            drain.at[4], sib_recv.at[a, d - 1, k, side], ep, sibling,
        )

    def place(k):
        for side in (1, 0):
            at = (k + STEPS * side) * chunk
            for a in range(2):
                placed = jnp.dot(
                    put[...], toks[a, :, cols(base + at, chunk)], preferred_element_type=F32
                ).astype(BF16).reshape(n_ep, cap, chunk)
                sends[a, :, :, cols(at, chunk)] = placed
                rows_v[a, ep, :, cols(base + at, chunk)] = sends[a, ep, :, cols(at, chunk)]

    def send_out(k):
        @pl.when(is_end)
        def _():
            for side in (1, 0):
                for a in range(2):
                    for d in near:
                        direct(a, d, k, side).start()

            @pl.when(k == STEPS - 1)
            def _():
                for a in range(2):
                    for d in far:
                        direct(a, d, k, 1 - upper, 1).start()

        @pl.when(is_inner)
        def _():
            for a in range(2):
                for d in far:
                    direct(a, d, k, upper).start()
            for a in range(2):
                for d in near:
                    direct(a, d, k, 0).start()

            @pl.when(k == STEPS - 1)
            def _():
                for a in range(2):
                    for d in near:
                        direct(a, d, k, 1, 1).start()

    loads[0].wait()
    loads[1].wait()
    place(0)
    entered()
    send_out(0)

    def place_step(k, carry):
        place(k)
        send_out(k)
        return carry

    lax.fori_loop(1, STEPS, place_step, 0)

    lane = lax.broadcasted_iota(jnp.int32, (tokens, capp), 1)
    lane_f = lane.astype(F32)
    for e in range(n_ep):
        weight = jnp.zeros((tokens, capp), F32)
        for k in range(top):
            hit = jnp.logical_and(lane_f == slot_c[k] - float(e * cap), lane < cap)
            weight = weight + jnp.where(hit, comb_c[k], 0.0)
        cs[e] = jnp.sum(weight, axis=0, keepdims=True)
    c_sends = []
    for d in range(1, n_ep):
        p = peer_of(ep, d, n_ep)
        copy = remote(cs.at[p], c_in.at[ep], c_s.at[d - 1], c_r.at[d - 1], p, tp)
        copy.start()
        c_sends.append(copy)
    c_in[ep] = cs[ep]
    pick[...] = one_hot(
        lax.broadcasted_iota(jnp.int32, (tokens, rows), 1).astype(F32), slot_c
    )
    square[...] = jnp.zeros_like(square)
    acc_g[...] = jnp.zeros_like(acc_g)
    acc_u[...] = jnp.zeros_like(acc_u)
    acc_h[...] = jnp.zeros_like(acc_h)
    loads[2].wait()
    loads[3].wait()
    other = (1 - core) * half
    for a in range(2):
        def own_step(j, carry, a=a):
            part = cols(other + j * (half // 4), half // 4)
            rows_v[a, ep, :, part] = jnp.dot(
                own_put, toks[a, :, part], preferred_element_type=F32
            ).astype(BF16)
            return carry

        lax.fori_loop(0, 4, own_step, 0)
    for load in loads[4:]:
        load.wait()

    def accumulate(h, k):
        parts = [cols(h * half + (k + STEPS * side) * chunk, chunk) for side in range(2)]

        def source(a, part):
            return rows_v[a, :, :, part].reshape(rows, chunk)

        for acc, w in ((acc_g, wg), (acc_u, wu)):
            acc[...] += jnp.dot(
                source(0, parts[0]), w[parts[0], :], preferred_element_type=F32
            ) + jnp.dot(source(0, parts[1]), w[parts[1], :], preferred_element_type=F32)
        acc_h[...] += dot_nt(source(1, parts[0]), wd[:, parts[0]]) + dot_nt(
            source(1, parts[1]), wd[:, parts[1]]
        )

    def taken(ds, k, side, *targets):
        for a in range(2):
            for d in ds:
                direct(a, d, k, side).wait_recv()
                for slot, target in targets:
                    along(a, d, k, side, slot, target).start()
                to_sibling(a, d, k, side).start()

    def finish(k):
        accumulate(core, k)
        for a in range(2):
            for side in range(2):
                for d in range(1, n_ep):
                    to_sibling(a, d, k, side).wait_recv()
        accumulate(1 - core, k)

    def arrive(k, carry):
        @pl.when(jnp.logical_and(is_end, k < STEPS - 1))
        def _():
            taken(near, k, 1, (2, inward))

        @pl.when(jnp.logical_and(is_end, k == STEPS - 1))
        def _():
            taken(near, k, 1)

        @pl.when(is_end)
        def _():
            @pl.when(k > 0)
            def _():
                taken(far, k - 1, upper)

            taken(near, k, 0)

            @pl.when(k > 0)
            def _():
                taken(far, k - 1, 1 - upper)

        @pl.when(is_inner)
        def _():
            taken(far, k, upper, (2, inward), (3, outward))

            @pl.when(k > 0)
            def _():
                taken(near, k - 1, 1)

            taken(near, k, 0)

        @pl.when(jnp.logical_and(is_inner, k < STEPS - 1))
        def _():
            taken(far, k, 1 - upper, (3, outward))

        @pl.when(jnp.logical_and(is_inner, k == STEPS - 1))
        def _():
            taken(near, k, 1)
            taken(far, k, 1 - upper)

        @pl.when(k > 0)
        def _():
            finish(k - 1)

        return carry

    lax.fori_loop(0, STEPS, arrive, 0)

    @pl.when(is_end)
    def _():
        taken(far, STEPS - 1, upper)
        taken(far, STEPS - 1, 1 - upper)

    finish(STEPS - 1)
    for copy in c_sends:
        copy.wait_recv()

    for p in range(n_ep):
        part = pl.ds(p * cap, cap)
        weight = jnp.broadcast_to(c_in[p], (LANES, capp)).T[:cap, :1]
        gate, up, grad = acc_g[part, :], acc_u[part, :], acc_h[part, :]
        sig = jax.nn.sigmoid(gate)
        silu = gate * sig
        hidden = silu * up
        score = jnp.sum(grad * hidden.astype(BF16).astype(F32), axis=1, keepdims=True)
        square[:cap, :] = jnp.broadcast_to(score, (cap, LANES))
        sc_in[tp, p] = square[...].T[:1, :]
        weighted = weight * grad
        hid[part, :] = (weight * hidden).astype(BF16)
        ggu[part, :units] = (weighted * up * sig * (1.0 + gate * (1.0 - sig))).astype(BF16)
        ggu[part, units:] = (weighted * silu).astype(BF16)

    def partial(share):
        part = pl.ds(pl.multiple_of(share * width, width), width)
        return dot_nt(ggu[:, :units], wg[part, :]) + dot_nt(ggu[:, units:], wu[part, :])

    sc_sends = []
    for k in range(1, n_tp):
        copy = remote(
            sc_in.at[tp], sc_in.at[tp], sc_s.at[k - 1], sc_r.at[k - 1],
            ep, lax.rem(tp + k, n_tp),
        )
        copy.start()
        sc_sends.append(copy)

    pairs, pair = nz // 2, z // 2
    owners = []
    for m in range(1, pairs):
        them = peer_of(pair, m, pairs)
        odd = lax.rem(them, 2)
        owners += [(m, 2 * them + odd), (m, 2 * them + 1 - odd)]
    n_far = 2 * len(owners)
    side, own = n_far, n_far + 1
    order = [q for _, q in owners[:1]] + [2 * pair + 1 - lax.rem(z, 2)]
    order += [q for _, q in owners[1:]] + [z]
    split = width // 2
    halves, moves = {}, {}

    def give_half(i):
        first[i] = partial(2 * order[i] + 1 - core).astype(BF16)
        halves[i] = remote(first.at[i], first_in.at[i], s1.at[i], r1.at[i], ep, sibling)
        halves[i].start()

    def spread(n):
        for d in range(1, n_ep):
            p = peer_of(ep, d, n_ep)
            copy = remote(
                second.at[n, p], second_in.at[n, ep], s2.at[n, d - 1], r2.at[n, d - 1], p, tp
            )
            copy.start()
            moves[n, d] = copy

    crossing = remote(across_v, across_in, sa, ra, ep, across)

    def join(i):
        total = partial(2 * order[i] + core)
        halves[i].wait_recv()
        total = total + first_in[i].astype(F32)
        low, high = total[:, :split], total[:, split:].astype(BF16).reshape(second.shape[1:])
        if i == 1:
            across_v[...] = low.astype(BF16)
            crossing.start()
            second[side] = high
        elif i < nz - 1:
            n = 2 * max(i - 1, 0)
            second[n] = low.astype(BF16).reshape(second.shape[1:])
            spread(n)
            second[n + 1] = high
            spread(n + 1)
        else:
            own_total[...] = low
            second[own + 1] = high
            spread(side)
            spread(own + 1)

    for i in range(nz):
        give_half(i)
        if i:
            join(i - 1)
    join(nz - 1)

    def tile(t):
        return pl.ds(pl.multiple_of(t * width, width), width)

    def gate_up_step(t, carry):
        both = lax.dot_general(
            rows_v[0, :, :, tile(t)].reshape(rows, width), ggu[...],
            (((0,), (0,)), ((), ())), preferred_element_type=F32,
        ).astype(BF16)
        gate_out[tile(t), :] = both[:, :units]
        up_out[tile(t), :] = both[:, units:]
        return carry

    hidden_t = hid[...].T

    def down_step(t, carry):
        down_out[:, tile(t)] = jnp.dot(
            hidden_t, rows_v[1, :, :, tile(t)].reshape(rows, width),
            preferred_element_type=F32,
        ).astype(BF16)
        return carry

    def gather_tokens(n):
        for d in range(1, n_ep):
            moves[n, d].wait_recv()
        second_in[n, ep] = second[n, ep]
        return jnp.dot(
            pick[...], second_in[n].reshape(rows, split), preferred_element_type=F32
        )

    def to_collector(n):
        return remote(third.at[n], third_in.at[n], s3.at[n], r3.at[n], ep, across)

    def to_owner(n):
        m, q = owners[n // 2]
        slot = 2 * (m - 1) + n % 2
        return remote(
            third.at[n], final_in.at[slot], s4.at[n], r4.at[slot], ep, 2 * q + core
        )

    def gather_far(n):
        summed = gather_tokens(n)

        @pl.when(is_end)
        def _():
            third[n] = summed.astype(BF16)
            to_collector(n).start()

        @pl.when(is_inner)
        def _():
            held[n] = summed

    def collect(n):
        @pl.when(is_inner)
        def _():
            to_collector(n).wait_recv()
            third[n] = (held[n] + third_in[n].astype(F32)).astype(BF16)
            to_owner(n).start()

    def gate_up(part):
        lax.fori_loop(part * n_tp // 2, (part + 1) * n_tp // 2, gate_up_step, 0)

    def share_scores():
        for copy in sc_sends:
            copy.wait_recv()
        summed = sc_in[0]
        for t in range(1, n_tp):
            summed = summed + sc_in[t]
        tot[...] = summed
        for d in range(1, n_ep):
            p = peer_of(ep, d, n_ep)
            copy = remote(tot.at[p], tot_in.at[ep], tot_s.at[d - 1], tot_r.at[d - 1], p, tp)
            copy.start()
            tot_sends.append(copy)
        tot_in[ep] = tot[ep]

    def cross():
        crossing.wait_recv()
        total = own_total[...] + across_in[...].astype(F32)
        second[own] = total.astype(BF16).reshape(second.shape[1:])
        spread(own)

    def down(part):
        lax.fori_loop(part * n_tp // 2, (part + 1) * n_tp // 2, down_step, 0)

    tot_sends = []
    work = [
        lambda: gate_up(0), lambda: gate_up(1), share_scores, cross,
        lambda: down(0), lambda: down(1),
    ]
    for n in range(n_far):
        gather_far(n)
        for job in work[2 * n : 2 * n + 2]:
            job()
        if n:
            collect(n - 1)
    side_copy = remote(
        third.at[side], final_in.at[2 * (pairs - 1)],
        s4.at[side], r4.at[2 * (pairs - 1)], ep, across,
    )
    third[side] = gather_tokens(side).astype(BF16)
    side_copy.start()
    collect(n_far - 1)
    for copy in tot_sends:
        copy.wait_recv()
    score_r = [jnp.zeros((1, tokens), F32) for _ in range(top)]
    for e in range(n_ep):
        column = jnp.broadcast_to(tot_in[e], (LANES, capp)).T[:cap, :1]
        index = (lax.broadcasted_iota(jnp.int32, (cap, tokens), 0) + e * cap).astype(F32)
        for k in range(top):
            score_r[k] = score_r[k] + jnp.sum(
                jnp.where(index == tab[k : k + 1, :], column, 0.0), axis=0, keepdims=True
            )
    group = jnp.zeros((1, tokens), F32)
    for k in range(top):
        inner_out[k : k + 1, :] = gates[...] * score_r[k]
        group = group + inner[k : k + 1, :] * score_r[k]
    group_out[...] = group

    def final_copy(slot):
        return remote(
            third.at[0], final_in.at[slot], s4.at[0], r4.at[slot], ep, across
        )

    high, low = gather_tokens(own + 1), gather_tokens(own)
    side_copy.wait_recv()
    high = high + final_in[2 * (pairs - 1)].astype(F32)
    for m in range(pairs - 1):
        final_copy(2 * m).wait_recv()
        low = low + final_in[2 * m].astype(F32)
        final_copy(2 * m + 1).wait_recv()
        high = high + final_in[2 * m + 1].astype(F32)
    out[:, :split] = low.astype(BF16)
    out[:, split:] = high.astype(BF16)

    def drained(ref, slot):
        remote(ref, ref, drain.at[slot], drain.at[slot], ep, sibling).wait_send()

    @pl.when(is_end)
    def _():
        drained(sends.at[:, : len(near)], 0)
        if far:
            drained(sends.at[:, : len(far), :, :chunk], 1)
        drained(rows_v.at[:, : len(near), :, : half // 2 - chunk], 2)

    @pl.when(is_inner)
    def _():
        drained(sends.at[:, : n_ep - 1, :, : half // 2], 0)
        drained(sends.at[:, : len(near), :, :chunk], 1)
        if far:
            drained(rows_v.at[:, : len(far), :, : half // 2], 2)
            drained(rows_v.at[:, : len(far), :, : half - chunk], 3)

    drained(rows_v.at[:, : n_ep - 1, :, :half], 4)
    for copy in c_sends + sc_sends + tot_sends + list(halves.values()) + list(moves.values()):
        copy.wait_send()
    crossing.wait_send()
    side_copy.wait_send()

    @pl.when(is_end)
    def _():
        for n in range(n_far):
            to_collector(n).wait_send()

    @pl.when(is_inner)
    def _():
        for n in range(n_far):
            to_owner(n).wait_send()


def layer(n_ep, n_tp, cap, route, gates, inner, tokens, cotangent, wg, wu, wd):
    vmem = pl.BlockSpec(memory_space=pltpu.VMEM)
    any_spec = pl.BlockSpec(memory_space=pl.ANY)
    nz = n_tp // 2
    count, model = tokens.shape
    rows, units = n_ep * cap, wg.shape[1]
    width, half = model // n_tp, model // 2
    capp = -(-cap // LANES) * LANES
    dma = pltpu.SemaphoreType.DMA
    return pl.pallas_call(
        functools.partial(layer_kernel, n_ep, n_tp, cap),
        out_shape=(
            pltpu.VMEM((count, width), BF16),
            pltpu.VMEM(gates.shape, F32),
            pltpu.VMEM(inner.shape, F32),
            pltpu.VMEM(wg.shape, BF16),
            pltpu.VMEM(wu.shape, BF16),
            pltpu.VMEM(wd.shape, BF16),
        ),
        in_specs=[vmem] * 3 + [any_spec] * 5,
        out_specs=(vmem,) * 6,
        scratch_shapes=[
            pltpu.VMEM((2, count, model), BF16),
            pltpu.VMEM((2, n_ep, cap, half), BF16),
            pltpu.VMEM((2, n_ep, cap, model), BF16),
            pltpu.VMEM(wg.shape, BF16),
            pltpu.VMEM(wu.shape, BF16),
            pltpu.VMEM(wd.shape, BF16),
            pltpu.VMEM((8, count), F32),
            pltpu.VMEM((rows, count), BF16),
            pltpu.VMEM((count, rows), BF16),
            pltpu.VMEM((n_ep, 1, capp), F32),
            pltpu.VMEM((n_ep, 1, capp), F32),
            pltpu.VMEM((capp, LANES), F32),
            pltpu.VMEM((n_tp, n_ep, 1, capp), F32),
            pltpu.VMEM((n_ep, 1, capp), F32),
            pltpu.VMEM((n_ep, 1, capp), F32),
            pltpu.VMEM((rows, units), F32),
            pltpu.VMEM((rows, units), F32),
            pltpu.VMEM((rows, units), F32),
            pltpu.VMEM((rows, 2 * units), BF16),
            pltpu.VMEM((rows, units), BF16),
            pltpu.VMEM((nz, rows, width), BF16),
            pltpu.VMEM((nz, rows, width), BF16),
            pltpu.VMEM((2 * nz - 1, n_ep, cap, width // 2), BF16),
            pltpu.VMEM((2 * nz - 1, n_ep, cap, width // 2), BF16),
            pltpu.VMEM((rows, width // 2), BF16),
            pltpu.VMEM((rows, width // 2), BF16),
            pltpu.VMEM((rows, width // 2), F32),
            pltpu.VMEM((2 * nz - 3, count, width // 2), BF16),
            pltpu.VMEM((2 * nz - 4, count, width // 2), BF16),
            pltpu.VMEM((2 * nz - 4, count, width // 2), F32),
            pltpu.VMEM((nz - 1, count, width // 2), BF16),
            dma((7,)),
            dma((5,)),
            dma((2, n_ep - 1, STEPS, 2)),
            dma((2, n_ep - 1, STEPS, 2)),
            dma((n_ep - 1,)), dma((n_ep - 1,)),
            dma((n_tp - 1,)), dma((n_tp - 1,)),
            dma((n_ep - 1,)), dma((n_ep - 1,)),
            dma((nz,)), dma((nz,)),
            dma((2 * nz - 1, n_ep - 1)), dma((2 * nz - 1, n_ep - 1)),
            dma((2 * nz - 4,)), dma((2 * nz - 4,)),
            dma((2 * nz - 3,)), dma((nz - 1,)),
            dma, dma,
        ],
        compiler_params=pltpu.CompilerParams(
            collective_id=0, has_side_effects=True, vmem_limit_bytes=54 * 1024 * 1024
        ),
    )(route, gates, inner, tokens, cotangent, wg, wu, wd)


def deliver_kernel(count, *refs):
    sems = refs[-1]
    copies = [
        pltpu.make_async_copy(refs[i], refs[count + i], sems.at[i]) for i in range(count)
    ]
    for copy in copies:
        copy.start()
    for copy in copies:
        copy.wait()


def deliver(*arrays):
    count = len(arrays)
    return pl.pallas_call(
        functools.partial(deliver_kernel, count),
        out_shape=tuple(jax.ShapeDtypeStruct(a.shape, a.dtype) for a in arrays),
        in_specs=[pl.BlockSpec(memory_space=pltpu.VMEM)] * count,
        out_specs=(pl.BlockSpec(memory_space=pl.ANY),) * count,
        scratch_shapes=[pltpu.SemaphoreType.DMA((count,))],
        compiler_params=pltpu.CompilerParams(vmem_limit_bytes=4 * 1024 * 1024),
    )(*arrays)


def per_device(tokens, cotangent, routing, group_gate, inner_gate, w_gate, w_up, w_down):
    n_ep, n_tp = lax.axis_size("ep"), lax.axis_size("tp")
    cap = tokens.shape[0] * routing.shape[1] * 5 // (4 * n_ep)
    results = layer(
        n_ep, n_tp, cap, routing.T, group_gate[None], inner_gate.T,
        tokens, cotangent, w_gate[0], w_up[0], w_down[0],
    )
    token_grad, group_grad, inner_grad, gate_grad, upper_grad, down_grad = deliver(*[
        pltpu.with_memory_space_constraint(r, pltpu.VMEM) for r in results
    ])
    return (
        token_grad,
        group_grad[0],
        inner_grad.T,
        gate_grad[None],
        upper_grad[None],
        down_grad[None],
    )


def solution(mesh):
    return jax.shard_map(
        per_device,
        mesh=mesh,
        in_specs=(
            P("ep", None),
            P("ep", None),
            P("ep", None),
            P("ep"),
            P("ep", None),
            P("ep", None, "tp"),
            P("ep", None, "tp"),
            P("ep", "tp", None),
        ),
        out_specs=(
            P("ep", "tp"),
            P("ep"),
            P("ep", None),
            P("ep", None, "tp"),
            P("ep", None, "tp"),
            P("ep", "tp", None),
        ),
        check_vma=False,
    )
```

```python
import functools

import jax
import jax.numpy as jnp
from jax import lax
from jax.experimental import pallas as pl
from jax.experimental.pallas import tpu as pltpu
from jax.sharding import PartitionSpec as P

LANES = 128
STEPS = 4
BF16 = jnp.bfloat16
F32 = jnp.float32


def peer_of(me, d, n):
    if n & (n - 1):
        return lax.rem(2 * n + d - me, n)
    out, bit = me, 1
    while bit < n:
        if d & bit:
            out = out + bit * (1 - 2 * lax.rem(me // bit, 2))
        bit *= 2
    return out


def barrier(partners):
    sem = pltpu.get_barrier_semaphore()
    for ep, tp in partners:
        pl.semaphore_signal(
            sem, inc=1, device_id=(ep, tp), device_id_type=pl.DeviceIdType.MESH
        )
    return lambda: pl.semaphore_wait(sem, len(partners))


def remote(src, dst, send, recv, ep, tp):
    return pltpu.make_async_remote_copy(
        src_ref=src,
        dst_ref=dst,
        send_sem=send,
        recv_sem=recv,
        device_id=(ep, tp),
        device_id_type=pl.DeviceIdType.MESH,
    )


def dot_nt(a, b):
    return lax.dot_general(a, b, (((1,), (1,)), ((), ())), preferred_element_type=F32)


def layer_kernel(n_ep, n_tp, cap, route, gates, inner, tok_hbm, cot_hbm, wg_hbm, wu_hbm, wd_hbm,
                 out, group_out, inner_out, gate_out, up_out, down_out,
                 toks, sends, rows_v, wg, wu, wd, tab, put, pick,
                 cs, c_in, square, sc_in, tot, tot_in,
                 acc_g, acc_u, acc_h, ggu, hid,
                 first, first_in, second, second_in, across_v, across_in, own_total,
                 third, third_in, held, final_in,
                 local, drain, recv, sib_recv, c_s, c_r, sc_s, sc_r, tot_s, tot_r,
                 s1, r1, s2, r2, s3, r3, s4, r4, sa, ra):
    ep, tp = lax.axis_index("ep"), lax.axis_index("tp")
    core = lax.rem(tp, 2)
    z = tp // 2
    nz = n_tp // 2
    sibling = tp + 1 - 2 * core
    across = tp + 2 - 4 * lax.rem(z, 2)
    spot = lax.rem(z, 4)
    is_end = jnp.logical_or(spot == 0, spot == 3)
    is_inner = jnp.logical_not(is_end)
    upper = spot // 2
    inward = tp + 2 - 4 * upper
    outward = tp - 2 + 4 * upper
    tokens, model = toks.shape[1], toks.shape[2]
    top = route.shape[0]
    half = model // 2
    chunk = half // (2 * STEPS)
    base = core * half
    rows = n_ep * cap
    capp = cs.shape[2]
    units = wg.shape[1]
    width = out.shape[1]
    near = [d for d in range(1, n_ep) if not d & (d - 1)]
    far = [d for d in range(1, n_ep) if d & (d - 1)]
    everyone = [(peer_of(ep, d, n_ep), tp) for d in range(1, n_ep)]
    everyone += [(ep, lax.rem(tp + k, n_tp)) for k in range(1, n_tp)]

    def cols(start, size):
        return pl.ds(pl.multiple_of(start, LANES), size)

    loads = []
    for h in (core, 1 - core):
        for a, src in enumerate((tok_hbm, cot_hbm)):
            part = cols(h * half, half)
            loads.append(pltpu.make_async_copy(
                src.at[:, part], toks.at[a, :, part], local.at[len(loads)]
            ))
    for src, dst in ((wg_hbm, wg), (wu_hbm, wu), (wd_hbm, wd)):
        loads.append(pltpu.make_async_copy(src, dst, local.at[len(loads)]))
    for load in loads:
        load.start()
    entered = barrier(everyone)

    route_v = route[...]
    expert = lax.broadcasted_iota(jnp.int32, (-(-n_ep // 16) * 16, tokens), 0)
    names = jnp.zeros(expert.shape, F32)
    for k in range(top):
        names = names + jnp.where(route_v[k : k + 1] == expert, 1.0, 0.0)
    earlier = jnp.where(
        lax.broadcasted_iota(jnp.int32, (tokens, tokens), 0)
        < lax.broadcasted_iota(jnp.int32, (tokens, tokens), 1), 1.0, 0.0,
    ).astype(BF16)
    rank = jnp.dot(names.astype(BF16), earlier, preferred_element_type=F32)
    place_of = (expert * cap).astype(F32) + rank
    tab[...] = jnp.zeros_like(tab)
    slot_r = []
    for k in range(top):
        slot = jnp.sum(
            jnp.where(route_v[k : k + 1] == expert, place_of, 0.0), axis=0, keepdims=True
        )
        slot_r.append(slot)
        tab[k : k + 1, :] = slot
        tab[top + k : top + k + 1, :] = gates[...] * inner[k : k + 1, :]
    turned = tab[...].T
    slot_c = [turned[:, k : k + 1] for k in range(top)]
    comb_c = [turned[:, top + k : top + k + 1] for k in range(top)]

    def one_hot(index, slots):
        hit = index == slots[0]
        for slot in slots[1:]:
            hit = jnp.logical_or(hit, index == slot)
        return jnp.where(hit, 1.0, 0.0).astype(BF16)

    put[...] = one_hot(
        lax.broadcasted_iota(jnp.int32, (rows, tokens), 0).astype(F32), slot_r
    )
    own_put = one_hot(
        (lax.broadcasted_iota(jnp.int32, (cap, tokens), 0) + ep * cap).astype(F32), slot_r
    )

    def piece(a, p, k, side):
        return rows_v.at[a, p, :, cols(base + (k + STEPS * side) * chunk, chunk)]

    def direct(a, d, k, side, slot=0):
        p = peer_of(ep, d, n_ep)
        return remote(
            sends.at[a, p, :, cols((k + STEPS * side) * chunk, chunk)],
            piece(a, ep, k, side),
            drain.at[slot], recv.at[a, d - 1, k, side], p, tp,
        )

    def along(a, d, k, side, slot, target):
        p = peer_of(ep, d, n_ep)
        return remote(
            piece(a, p, k, side), piece(a, p, k, side),
            drain.at[slot], recv.at[a, d - 1, k, side], ep, target,
        )

    def to_sibling(a, d, k, side):
        p = peer_of(ep, d, n_ep)
        return remote(
            piece(a, p, k, side), piece(a, p, k, side),
            drain.at[4], sib_recv.at[a, d - 1, k, side], ep, sibling,
        )

    def place(k):
        for side in (1, 0):
            at = (k + STEPS * side) * chunk
            for a in range(2):
                placed = jnp.dot(
                    put[...], toks[a, :, cols(base + at, chunk)], preferred_element_type=F32
                ).astype(BF16).reshape(n_ep, cap, chunk)
                sends[a, :, :, cols(at, chunk)] = placed
                rows_v[a, ep, :, cols(base + at, chunk)] = sends[a, ep, :, cols(at, chunk)]

    def send_out(k):
        @pl.when(is_end)
        def _():
            for a in range(2):
                for d in near:
                    direct(a, d, k, 1).start()

            @pl.when(k == STEPS - 1)
            def _():
                for d in far:
                    direct(0, d, k, 1 - upper, 1).start()

            for a in range(2):
                for d in near:
                    direct(a, d, k, 0).start()

        @pl.when(is_inner)
        def _():
            for a in range(2):
                for d in far:
                    direct(a, d, k, upper).start()

            @pl.when(k > 0)
            def _():
                for a in range(2):
                    for d in near:
                        direct(a, d, k - 1, 0).start()

            @pl.when(k == STEPS - 1)
            def _():
                for a in range(2):
                    for d in near:
                        direct(a, d, k, 0).start()
                for d in near:
                    direct(0, d, k, 1, 1).start()

    loads[0].wait()
    loads[1].wait()
    place(0)
    entered()
    send_out(0)

    def place_step(k, carry):
        place(k)
        send_out(k)
        return carry

    lax.fori_loop(1, STEPS, place_step, 0)

    lane = lax.broadcasted_iota(jnp.int32, (tokens, capp), 1)
    lane_f = lane.astype(F32)
    for e in range(n_ep):
        weight = jnp.zeros((tokens, capp), F32)
        for k in range(top):
            hit = jnp.logical_and(lane_f == slot_c[k] - float(e * cap), lane < cap)
            weight = weight + jnp.where(hit, comb_c[k], 0.0)
        cs[e] = jnp.sum(weight, axis=0, keepdims=True)
    c_sends = []
    for d in range(1, n_ep):
        p = peer_of(ep, d, n_ep)
        copy = remote(cs.at[p], c_in.at[ep], c_s.at[d - 1], c_r.at[d - 1], p, tp)
        copy.start()
        c_sends.append(copy)
    c_in[ep] = cs[ep]
    pick[...] = one_hot(
        lax.broadcasted_iota(jnp.int32, (tokens, rows), 1).astype(F32), slot_c
    )
    square[...] = jnp.zeros_like(square)
    acc_g[...] = jnp.zeros_like(acc_g)
    acc_u[...] = jnp.zeros_like(acc_u)
    acc_h[...] = jnp.zeros_like(acc_h)
    loads[2].wait()
    loads[3].wait()
    other = (1 - core) * half
    for a in range(2):
        def own_step(j, carry, a=a):
            part = cols(other + j * (half // 4), half // 4)
            rows_v[a, ep, :, part] = jnp.dot(
                own_put, toks[a, :, part], preferred_element_type=F32
            ).astype(BF16)
            return carry

        lax.fori_loop(0, 4, own_step, 0)
    for load in loads[4:]:
        load.wait()

    def accumulate(h, k, side):
        part = cols(h * half + (k + STEPS * side) * chunk, chunk)
        source = [rows_v[a, :, :, part].reshape(rows, chunk) for a in range(2)]
        for acc, w in ((acc_g, wg), (acc_u, wu)):
            acc[...] += jnp.dot(source[0], w[part, :], preferred_element_type=F32)
        acc_h[...] += dot_nt(source[1], wd[:, part])

    def taken(ds, k, side, *targets, arrays=(0, 1)):
        for a in arrays:
            for d in ds:
                direct(a, d, k, side).wait_recv()
                for slot, target in targets:
                    along(a, d, k, side, slot, target).start()
                to_sibling(a, d, k, side).start()

    def finish(*pieces):
        for k, side in pieces:
            accumulate(core, k, side)
        return pieces

    def finish_other(pieces):
        for k, side in pieces:
            for a in range(2):
                for d in range(1, n_ep):
                    to_sibling(a, d, k, side).wait_recv()
            accumulate(1 - core, k, side)

    def arrive_end(k, carry):
        @pl.when(k < STEPS - 1)
        def _():
            taken(near, k, 1, (2, inward))

        @pl.when(k == STEPS - 1)
        def _():
            taken(near, k, 1, (2, inward), arrays=(1,))
            taken(near, k, 1, arrays=(0,))

        @pl.when(k > 0)
        def _():
            taken(far, k - 1, 1 - upper)

        taken(far, k, upper)

        @pl.when(k > 0)
        def _():
            finish((k - 1, 1 - upper))

        @pl.when(k == STEPS - 1)
        def _():
            taken(far, k, 1 - upper)

        @pl.when(k > 0)
        def _():
            finish_other([(k - 1, 1 - upper)])

        taken(near, k, 0)
        finish((k, upper))

        @pl.when(k == STEPS - 1)
        def _():
            finish((k, 1 - upper))

        finish_other([(k, upper)])
        return carry

    def arrive_inner(k, carry):
        taken(near, k, 0)

        @pl.when(k < STEPS - 2)
        def _():
            taken(far, k + 1, 1 - upper, (3, outward))

        @pl.when(k == STEPS - 2)
        def _():
            taken(far, k + 1, 1 - upper, (3, outward), arrays=(1,))
            taken(far, k + 1, 1 - upper, arrays=(0,))

        @pl.when(k == STEPS - 1)
        def _():
            finish_other(finish((k, 0)))
            taken(near, k, 1)
            finish_other(finish((k, 1)))

        @pl.when(k < STEPS - 1)
        def _():
            taken(near, k, 1)
            done = finish((k, 0), (k, 1))

            @pl.when(k < STEPS - 2)
            def _():
                taken(far, k + 2, upper, (2, inward), (3, outward))

            finish_other(done)

        return carry

    @pl.when(is_end)
    def _():
        lax.fori_loop(0, STEPS, arrive_end, 0)
        finish_other([(STEPS - 1, 1 - upper)])

    @pl.when(is_inner)
    def _():
        taken(far, 0, upper, (2, inward), (3, outward))
        taken(far, 1, upper, (2, inward), (3, outward))
        taken(far, 0, 1 - upper, (3, outward))
        lax.fori_loop(0, STEPS, arrive_inner, 0)

    for copy in c_sends:
        copy.wait_recv()

    for p in range(n_ep):
        part = pl.ds(p * cap, cap)
        weight = jnp.broadcast_to(c_in[p], (LANES, capp)).T[:cap, :1]
        gate, up, grad = acc_g[part, :], acc_u[part, :], acc_h[part, :]
        sig = jax.nn.sigmoid(gate)
        silu = gate * sig
        hidden = silu * up
        score = jnp.sum(grad * hidden.astype(BF16).astype(F32), axis=1, keepdims=True)
        square[:cap, :] = jnp.broadcast_to(score, (cap, LANES))
        sc_in[tp, p] = square[...].T[:1, :]
        weighted = weight * grad
        hid[part, :] = (weight * hidden).astype(BF16)
        ggu[part, :units] = (weighted * up * sig * (1.0 + gate * (1.0 - sig))).astype(BF16)
        ggu[part, units:] = (weighted * silu).astype(BF16)

    def partial(share):
        part = pl.ds(pl.multiple_of(share * width, width), width)
        return dot_nt(ggu[:, :units], wg[part, :]) + dot_nt(ggu[:, units:], wu[part, :])

    sc_sends = []
    for k in range(1, n_tp):
        copy = remote(
            sc_in.at[tp], sc_in.at[tp], sc_s.at[k - 1], sc_r.at[k - 1],
            ep, lax.rem(tp + k, n_tp),
        )
        copy.start()
        sc_sends.append(copy)

    pairs, pair = nz // 2, z // 2
    owners = []
    for m in range(1, pairs):
        them = peer_of(pair, m, pairs)
        odd = lax.rem(them, 2)
        owners += [(m, 2 * them + odd), (m, 2 * them + 1 - odd)]
    n_far = 2 * len(owners)
    side, own = n_far, n_far + 1
    order = [q for _, q in owners[:1]] + [2 * pair + 1 - lax.rem(z, 2)]
    order += [q for _, q in owners[1:]] + [z]
    split = width // 2
    halves, moves = {}, {}

    def give_half(i):
        first[i] = partial(2 * order[i] + 1 - core).astype(BF16)
        halves[i] = remote(first.at[i], first_in.at[i], s1.at[i], r1.at[i], ep, sibling)
        halves[i].start()

    def spread(n):
        for d in far + near:
            p = peer_of(ep, d, n_ep)
            copy = remote(
                second.at[n, p], second_in.at[n, ep], s2.at[n, d - 1], r2.at[n, d - 1], p, tp
            )
            copy.start()
            moves[n, d] = copy

    crossing = remote(across_v, across_in, sa, ra, ep, across)

    def join(i):
        total = partial(2 * order[i] + core)
        halves[i].wait_recv()
        total = total + first_in[i].astype(F32)
        low, high = total[:, :split], total[:, split:].astype(BF16).reshape(second.shape[1:])
        if i == 1:
            across_v[...] = low.astype(BF16)
            crossing.start()
            second[side] = high
        elif i < nz - 1:
            n = 2 * max(i - 1, 0)
            second[n] = low.astype(BF16).reshape(second.shape[1:])
            spread(n)
            second[n + 1] = high
            spread(n + 1)
        else:
            own_total[...] = low
            second[own + 1] = high
            spread(side)
            spread(own + 1)

    for i in range(nz):
        give_half(i)
        if i:
            join(i - 1)
    join(nz - 1)

    def tile(t):
        return pl.ds(pl.multiple_of(t * width, width), width)

    def gate_up_step(t, carry):
        both = lax.dot_general(
            rows_v[0, :, :, tile(t)].reshape(rows, width), ggu[...],
            (((0,), (0,)), ((), ())), preferred_element_type=F32,
        ).astype(BF16)
        gate_out[tile(t), :] = both[:, :units]
        up_out[tile(t), :] = both[:, units:]
        return carry

    hidden_t = hid[...].T

    def down_step(t, carry):
        down_out[:, tile(t)] = jnp.dot(
            hidden_t, rows_v[1, :, :, tile(t)].reshape(rows, width),
            preferred_element_type=F32,
        ).astype(BF16)
        return carry

    def gather_tokens(n):
        for d in range(1, n_ep):
            moves[n, d].wait_recv()
        second_in[n, ep] = second[n, ep]
        return jnp.dot(
            pick[...], second_in[n].reshape(rows, split), preferred_element_type=F32
        )

    def to_collector(n):
        return remote(third.at[n], third_in.at[n], s3.at[n], r3.at[n], ep, across)

    def to_owner(n):
        m, q = owners[n // 2]
        slot = 2 * (m - 1) + n % 2
        return remote(
            third.at[n], final_in.at[slot], s4.at[n], r4.at[slot], ep, 2 * q + core
        )

    def gather_far(n):
        summed = gather_tokens(n)

        @pl.when(is_end)
        def _():
            third[n] = summed.astype(BF16)
            to_collector(n).start()

        @pl.when(is_inner)
        def _():
            held[n] = summed

    def collect(n):
        @pl.when(is_inner)
        def _():
            to_collector(n).wait_recv()
            third[n] = (held[n] + third_in[n].astype(F32)).astype(BF16)
            to_owner(n).start()

    def gate_up(part):
        lax.fori_loop(part * n_tp // 2, (part + 1) * n_tp // 2, gate_up_step, 0)

    def share_scores():
        for copy in sc_sends:
            copy.wait_recv()
        summed = sc_in[0]
        for t in range(1, n_tp):
            summed = summed + sc_in[t]
        tot[...] = summed
        for d in range(1, n_ep):
            p = peer_of(ep, d, n_ep)
            copy = remote(tot.at[p], tot_in.at[ep], tot_s.at[d - 1], tot_r.at[d - 1], p, tp)
            copy.start()
            tot_sends.append(copy)
        tot_in[ep] = tot[ep]

    def cross():
        crossing.wait_recv()
        total = own_total[...] + across_in[...].astype(F32)
        second[own] = total.astype(BF16).reshape(second.shape[1:])
        spread(own)

    def down(part):
        lax.fori_loop(part * n_tp // 2, (part + 1) * n_tp // 2, down_step, 0)

    tot_sends = []
    work = [
        lambda: gate_up(0), lambda: gate_up(1), share_scores, cross,
        lambda: down(0), lambda: down(1),
    ]
    for n in range(n_far):
        gather_far(n)
        for job in work[2 * n : 2 * n + 2]:
            job()
        if n:
            collect(n - 1)
    side_copy = remote(
        third.at[side], final_in.at[2 * (pairs - 1)],
        s4.at[side], r4.at[2 * (pairs - 1)], ep, across,
    )
    third[side] = gather_tokens(side).astype(BF16)
    side_copy.start()
    collect(n_far - 1)
    for copy in tot_sends:
        copy.wait_recv()
    score_r = [jnp.zeros((1, tokens), F32) for _ in range(top)]
    for e in range(n_ep):
        column = jnp.broadcast_to(tot_in[e], (LANES, capp)).T[:cap, :1]
        index = (lax.broadcasted_iota(jnp.int32, (cap, tokens), 0) + e * cap).astype(F32)
        for k in range(top):
            score_r[k] = score_r[k] + jnp.sum(
                jnp.where(index == tab[k : k + 1, :], column, 0.0), axis=0, keepdims=True
            )
    group = jnp.zeros((1, tokens), F32)
    for k in range(top):
        inner_out[k : k + 1, :] = gates[...] * score_r[k]
        group = group + inner[k : k + 1, :] * score_r[k]
    group_out[...] = group

    def final_copy(slot):
        return remote(
            third.at[0], final_in.at[slot], s4.at[0], r4.at[slot], ep, across
        )

    high = gather_tokens(own + 1)
    side_copy.wait_recv()
    high = high + final_in[2 * (pairs - 1)].astype(F32)
    for m in range(pairs - 1):
        final_copy(2 * m + 1).wait_recv()
        high = high + final_in[2 * m + 1].astype(F32)
    out[:, split:] = high.astype(BF16)
    low = gather_tokens(own)
    for m in range(pairs - 1):
        final_copy(2 * m).wait_recv()
        low = low + final_in[2 * m].astype(F32)
    out[:, :split] = low.astype(BF16)

    def drained(ref, slot):
        remote(ref, ref, drain.at[slot], drain.at[slot], ep, sibling).wait_send()

    @pl.when(is_end)
    def _():
        drained(sends.at[:, : len(near)], 0)
        if far:
            drained(sends.at[0, : len(far), :, :chunk], 1)
        drained(rows_v.at[0, : len(near), :, : half - chunk], 2)

    @pl.when(is_inner)
    def _():
        drained(sends.at[:, : n_ep - 1, :, : half // 2], 0)
        drained(sends.at[0, : len(near), :, :chunk], 1)
        if far:
            drained(rows_v.at[:, : len(far), :, : half // 2], 2)
            drained(rows_v.at[0, : len(far), :, : model - chunk], 3)

    drained(rows_v.at[:, : n_ep - 1, :, :half], 4)
    for copy in c_sends + sc_sends + tot_sends + list(halves.values()) + list(moves.values()):
        copy.wait_send()
    crossing.wait_send()
    side_copy.wait_send()

    @pl.when(is_end)
    def _():
        for n in range(n_far):
            to_collector(n).wait_send()

    @pl.when(is_inner)
    def _():
        for n in range(n_far):
            to_owner(n).wait_send()


def layer(n_ep, n_tp, cap, route, gates, inner, tokens, cotangent, wg, wu, wd):
    vmem = pl.BlockSpec(memory_space=pltpu.VMEM)
    any_spec = pl.BlockSpec(memory_space=pl.ANY)
    nz = n_tp // 2
    count, model = tokens.shape
    rows, units = n_ep * cap, wg.shape[1]
    width, half = model // n_tp, model // 2
    capp = -(-cap // LANES) * LANES
    dma = pltpu.SemaphoreType.DMA
    return pl.pallas_call(
        functools.partial(layer_kernel, n_ep, n_tp, cap),
        out_shape=(
            pltpu.VMEM((count, width), BF16),
            pltpu.VMEM(gates.shape, F32),
            pltpu.VMEM(inner.shape, F32),
            pltpu.VMEM(wg.shape, BF16),
            pltpu.VMEM(wu.shape, BF16),
            pltpu.VMEM(wd.shape, BF16),
        ),
        in_specs=[vmem] * 3 + [any_spec] * 5,
        out_specs=(vmem,) * 6,
        scratch_shapes=[
            pltpu.VMEM((2, count, model), BF16),
            pltpu.VMEM((2, n_ep, cap, half), BF16),
            pltpu.VMEM((2, n_ep, cap, model), BF16),
            pltpu.VMEM(wg.shape, BF16),
            pltpu.VMEM(wu.shape, BF16),
            pltpu.VMEM(wd.shape, BF16),
            pltpu.VMEM((8, count), F32),
            pltpu.VMEM((rows, count), BF16),
            pltpu.VMEM((count, rows), BF16),
            pltpu.VMEM((n_ep, 1, capp), F32),
            pltpu.VMEM((n_ep, 1, capp), F32),
            pltpu.VMEM((capp, LANES), F32),
            pltpu.VMEM((n_tp, n_ep, 1, capp), F32),
            pltpu.VMEM((n_ep, 1, capp), F32),
            pltpu.VMEM((n_ep, 1, capp), F32),
            pltpu.VMEM((rows, units), F32),
            pltpu.VMEM((rows, units), F32),
            pltpu.VMEM((rows, units), F32),
            pltpu.VMEM((rows, 2 * units), BF16),
            pltpu.VMEM((rows, units), BF16),
            pltpu.VMEM((nz, rows, width), BF16),
            pltpu.VMEM((nz, rows, width), BF16),
            pltpu.VMEM((2 * nz - 1, n_ep, cap, width // 2), BF16),
            pltpu.VMEM((2 * nz - 1, n_ep, cap, width // 2), BF16),
            pltpu.VMEM((rows, width // 2), BF16),
            pltpu.VMEM((rows, width // 2), BF16),
            pltpu.VMEM((rows, width // 2), F32),
            pltpu.VMEM((2 * nz - 3, count, width // 2), BF16),
            pltpu.VMEM((2 * nz - 4, count, width // 2), BF16),
            pltpu.VMEM((2 * nz - 4, count, width // 2), F32),
            pltpu.VMEM((nz - 1, count, width // 2), BF16),
            dma((7,)),
            dma((5,)),
            dma((2, n_ep - 1, STEPS, 2)),
            dma((2, n_ep - 1, STEPS, 2)),
            dma((n_ep - 1,)), dma((n_ep - 1,)),
            dma((n_tp - 1,)), dma((n_tp - 1,)),
            dma((n_ep - 1,)), dma((n_ep - 1,)),
            dma((nz,)), dma((nz,)),
            dma((2 * nz - 1, n_ep - 1)), dma((2 * nz - 1, n_ep - 1)),
            dma((2 * nz - 4,)), dma((2 * nz - 4,)),
            dma((2 * nz - 3,)), dma((nz - 1,)),
            dma, dma,
        ],
        compiler_params=pltpu.CompilerParams(
            collective_id=0, has_side_effects=True, vmem_limit_bytes=54 * 1024 * 1024
        ),
    )(route, gates, inner, tokens, cotangent, wg, wu, wd)


def deliver_kernel(count, *refs):
    sems = refs[-1]
    copies = [
        pltpu.make_async_copy(refs[i], refs[count + i], sems.at[i]) for i in range(count)
    ]
    for copy in copies:
        copy.start()
    for copy in copies:
        copy.wait()


def deliver(*arrays):
    count = len(arrays)
    return pl.pallas_call(
        functools.partial(deliver_kernel, count),
        out_shape=tuple(jax.ShapeDtypeStruct(a.shape, a.dtype) for a in arrays),
        in_specs=[pl.BlockSpec(memory_space=pltpu.VMEM)] * count,
        out_specs=(pl.BlockSpec(memory_space=pl.ANY),) * count,
        scratch_shapes=[pltpu.SemaphoreType.DMA((count,))],
        compiler_params=pltpu.CompilerParams(vmem_limit_bytes=4 * 1024 * 1024),
    )(*arrays)


def per_device(tokens, cotangent, routing, group_gate, inner_gate, w_gate, w_up, w_down):
    n_ep, n_tp = lax.axis_size("ep"), lax.axis_size("tp")
    cap = tokens.shape[0] * routing.shape[1] * 5 // (4 * n_ep)
    results = layer(
        n_ep, n_tp, cap, routing.T, group_gate[None], inner_gate.T,
        tokens, cotangent, w_gate[0], w_up[0], w_down[0],
    )
    token_grad, group_grad, inner_grad, gate_grad, upper_grad, down_grad = deliver(*[
        pltpu.with_memory_space_constraint(r, pltpu.VMEM) for r in results
    ])
    return (
        token_grad,
        group_grad[0],
        inner_grad.T,
        gate_grad[None],
        upper_grad[None],
        down_grad[None],
    )


def solution(mesh):
    return jax.shard_map(
        per_device,
        mesh=mesh,
        in_specs=(
            P("ep", None),
            P("ep", None),
            P("ep", None),
            P("ep"),
            P("ep", None),
            P("ep", None, "tp"),
            P("ep", None, "tp"),
            P("ep", "tp", None),
        ),
        out_specs=(
            P("ep", "tp"),
            P("ep"),
            P("ep", None),
            P("ep", None, "tp"),
            P("ep", None, "tp"),
            P("ep", "tp", None),
        ),
        check_vma=False,
    )
```

```python
import functools

import jax
import jax.numpy as jnp
from jax import lax
from jax.experimental import pallas as pl
from jax.experimental.pallas import tpu as pltpu
from jax.sharding import PartitionSpec as P

LANES = 128
STEPS = 4
BF16 = jnp.bfloat16
F32 = jnp.float32


def peer_of(me, d, n):
    if n & (n - 1):
        return lax.rem(2 * n + d - me, n)
    out, bit = me, 1
    while bit < n:
        if d & bit:
            out = out + bit * (1 - 2 * lax.rem(me // bit, 2))
        bit *= 2
    return out


def barrier(partners):
    sem = pltpu.get_barrier_semaphore()
    for ep, tp in partners:
        pl.semaphore_signal(
            sem, inc=1, device_id=(ep, tp), device_id_type=pl.DeviceIdType.MESH
        )
    return lambda: pl.semaphore_wait(sem, len(partners))


def remote(src, dst, send, recv, ep, tp):
    return pltpu.make_async_remote_copy(
        src_ref=src,
        dst_ref=dst,
        send_sem=send,
        recv_sem=recv,
        device_id=(ep, tp),
        device_id_type=pl.DeviceIdType.MESH,
    )


def dot_nt(a, b):
    return lax.dot_general(a, b, (((1,), (1,)), ((), ())), preferred_element_type=F32)


def layer_kernel(n_ep, n_tp, cap, route, gates, inner, tok_hbm, cot_hbm, wg_hbm, wu_hbm, wd_hbm,
                 out, group_out, inner_out, gate_out, up_out, down_out,
                 toks, sends, rows_v, wg, wu, wd, tab, put, pick,
                 cs, c_in, square, sc_in, tot, tot_in,
                 acc_g, acc_u, acc_h, ggu, hid,
                 first, first_in, second, second_in, across_v, across_in, own_total,
                 third, third_in, held, final_in,
                 local, drain, recv, sib_recv, c_s, c_r, sc_s, sc_r, tot_s, tot_r,
                 s1, r1, s2, r2, s3, r3, s4, r4, sa, ra):
    ep, tp = lax.axis_index("ep"), lax.axis_index("tp")
    core = lax.rem(tp, 2)
    z = tp // 2
    nz = n_tp // 2
    sibling = tp + 1 - 2 * core
    across = tp + 2 - 4 * lax.rem(z, 2)
    spot = lax.rem(z, 4)
    is_end = jnp.logical_or(spot == 0, spot == 3)
    is_inner = jnp.logical_not(is_end)
    upper = spot // 2
    inward = tp + 2 - 4 * upper
    outward = tp - 2 + 4 * upper
    tokens, model = toks.shape[1], toks.shape[2]
    top = route.shape[0]
    half = model // 2
    chunk = half // (2 * STEPS)
    base = core * half
    rows = n_ep * cap
    capp = cs.shape[2]
    units = wg.shape[1]
    width = out.shape[1]
    near = [d for d in range(1, n_ep) if not d & (d - 1)]
    far = [d for d in range(1, n_ep) if d & (d - 1)]
    everyone = [(peer_of(ep, d, n_ep), tp) for d in range(1, n_ep)]
    everyone += [(ep, lax.rem(tp + k, n_tp)) for k in range(1, n_tp)]

    def cols(start, size):
        return pl.ds(pl.multiple_of(start, LANES), size)

    loads = []
    for h in (core, 1 - core):
        for a, src in enumerate((tok_hbm, cot_hbm)):
            part = cols(h * half, half)
            loads.append(pltpu.make_async_copy(
                src.at[:, part], toks.at[a, :, part], local.at[len(loads)]
            ))
    for src, dst in ((wg_hbm, wg), (wu_hbm, wu), (wd_hbm, wd)):
        loads.append(pltpu.make_async_copy(src, dst, local.at[len(loads)]))
    for load in loads:
        load.start()
    entered = barrier(everyone)

    route_v = route[...]
    expert = lax.broadcasted_iota(jnp.int32, (-(-n_ep // 16) * 16, tokens), 0)
    names = jnp.zeros(expert.shape, F32)
    for k in range(top):
        names = names + jnp.where(route_v[k : k + 1] == expert, 1.0, 0.0)
    earlier = jnp.where(
        lax.broadcasted_iota(jnp.int32, (tokens, tokens), 0)
        < lax.broadcasted_iota(jnp.int32, (tokens, tokens), 1), 1.0, 0.0,
    ).astype(BF16)
    rank = jnp.dot(names.astype(BF16), earlier, preferred_element_type=F32)
    place_of = (expert * cap).astype(F32) + rank
    tab[...] = jnp.zeros_like(tab)
    slot_r = []
    for k in range(top):
        slot = jnp.sum(
            jnp.where(route_v[k : k + 1] == expert, place_of, 0.0), axis=0, keepdims=True
        )
        slot_r.append(slot)
        tab[k : k + 1, :] = slot
        tab[top + k : top + k + 1, :] = gates[...] * inner[k : k + 1, :]
    turned = tab[...].T
    slot_c = [turned[:, k : k + 1] for k in range(top)]
    comb_c = [turned[:, top + k : top + k + 1] for k in range(top)]

    def one_hot(index, slots):
        hit = index == slots[0]
        for slot in slots[1:]:
            hit = jnp.logical_or(hit, index == slot)
        return jnp.where(hit, 1.0, 0.0).astype(BF16)

    put[...] = one_hot(
        lax.broadcasted_iota(jnp.int32, (rows, tokens), 0).astype(F32), slot_r
    )
    own_put = one_hot(
        (lax.broadcasted_iota(jnp.int32, (cap, tokens), 0) + ep * cap).astype(F32), slot_r
    )

    def piece(a, p, k, side):
        return rows_v.at[a, p, :, cols(base + (k + STEPS * side) * chunk, chunk)]

    def direct(a, d, k, side, slot=0):
        p = peer_of(ep, d, n_ep)
        return remote(
            sends.at[a, p, :, cols((k + STEPS * side) * chunk, chunk)],
            piece(a, ep, k, side),
            drain.at[slot], recv.at[a, d - 1, k, side], p, tp,
        )

    def along(a, d, k, side, slot, target):
        p = peer_of(ep, d, n_ep)
        return remote(
            piece(a, p, k, side), piece(a, p, k, side),
            drain.at[slot], recv.at[a, d - 1, k, side], ep, target,
        )

    def to_sibling(a, d, k, side):
        p = peer_of(ep, d, n_ep)
        return remote(
            piece(a, p, k, side), piece(a, p, k, side),
            drain.at[4], sib_recv.at[a, d - 1, k, side], ep, sibling,
        )

    def place(k):
        for side in (1, 0):
            at = (k + STEPS * side) * chunk
            for a in range(2):
                placed = jnp.dot(
                    put[...], toks[a, :, cols(base + at, chunk)], preferred_element_type=F32
                ).astype(BF16).reshape(n_ep, cap, chunk)
                sends[a, :, :, cols(at, chunk)] = placed
                rows_v[a, ep, :, cols(base + at, chunk)] = sends[a, ep, :, cols(at, chunk)]

    def send_out(k):
        @pl.when(is_end)
        def _():
            for a in range(2):
                for d in near:
                    direct(a, d, k, 1).start()

            @pl.when(k == STEPS - 1)
            def _():
                for d in far:
                    direct(0, d, k, 1 - upper, 1).start()

            for a in range(2):
                for d in near:
                    direct(a, d, k, 0).start()

        @pl.when(is_inner)
        def _():
            for a in range(2):
                for d in far:
                    direct(a, d, k, upper).start()

            @pl.when(k > 0)
            def _():
                for a in range(2):
                    for d in near:
                        direct(a, d, k - 1, 0).start()

            @pl.when(k == STEPS - 1)
            def _():
                for a in range(2):
                    for d in near:
                        direct(a, d, k, 0).start()
                for d in near:
                    direct(0, d, k, 1, 1).start()

    loads[0].wait()
    loads[1].wait()
    place(0)
    entered()
    send_out(0)

    def place_step(k, carry):
        place(k)
        send_out(k)
        return carry

    lax.fori_loop(1, STEPS, place_step, 0)

    lane = lax.broadcasted_iota(jnp.int32, (tokens, capp), 1)
    lane_f = lane.astype(F32)
    for e in range(n_ep):
        weight = jnp.zeros((tokens, capp), F32)
        for k in range(top):
            hit = jnp.logical_and(lane_f == slot_c[k] - float(e * cap), lane < cap)
            weight = weight + jnp.where(hit, comb_c[k], 0.0)
        cs[e] = jnp.sum(weight, axis=0, keepdims=True)
    c_sends = []
    for d in range(1, n_ep):
        p = peer_of(ep, d, n_ep)
        copy = remote(cs.at[p], c_in.at[ep], c_s.at[d - 1], c_r.at[d - 1], p, tp)
        copy.start()
        c_sends.append(copy)
    c_in[ep] = cs[ep]
    pick[...] = one_hot(
        lax.broadcasted_iota(jnp.int32, (tokens, rows), 1).astype(F32), slot_c
    )
    square[...] = jnp.zeros_like(square)
    acc_g[...] = jnp.zeros_like(acc_g)
    acc_u[...] = jnp.zeros_like(acc_u)
    acc_h[...] = jnp.zeros_like(acc_h)
    loads[2].wait()
    loads[3].wait()
    other = (1 - core) * half
    for a in range(2):
        def own_step(j, carry, a=a):
            part = cols(other + j * (half // 4), half // 4)
            rows_v[a, ep, :, part] = jnp.dot(
                own_put, toks[a, :, part], preferred_element_type=F32
            ).astype(BF16)
            return carry

        lax.fori_loop(0, 4, own_step, 0)
    for load in loads[4:]:
        load.wait()

    def accumulate(h, k, side):
        part = cols(h * half + (k + STEPS * side) * chunk, chunk)
        source = [rows_v[a, :, :, part].reshape(rows, chunk) for a in range(2)]
        for acc, w in ((acc_g, wg), (acc_u, wu)):
            acc[...] += jnp.dot(source[0], w[part, :], preferred_element_type=F32)
        acc_h[...] += dot_nt(source[1], wd[:, part])

    def taken(ds, k, side, *targets, arrays=(0, 1)):
        for a in arrays:
            for d in ds:
                direct(a, d, k, side).wait_recv()
                for slot, target in targets:
                    along(a, d, k, side, slot, target).start()
                to_sibling(a, d, k, side).start()

    def finish(*pieces):
        for k, side in pieces:
            accumulate(core, k, side)
        return pieces

    def finish_other(pieces):
        for k, side in pieces:
            for a in range(2):
                for d in range(1, n_ep):
                    to_sibling(a, d, k, side).wait_recv()
            accumulate(1 - core, k, side)

    def arrive_end(k, carry):
        @pl.when(k < STEPS - 1)
        def _():
            taken(near, k, 1, (2, inward))

        @pl.when(k == STEPS - 1)
        def _():
            taken(near, k, 1, (2, inward), arrays=(1,))
            taken(near, k, 1, arrays=(0,))

        @pl.when(k > 0)
        def _():
            taken(far, k - 1, 1 - upper)

        taken(far, k, upper)

        @pl.when(k > 0)
        def _():
            finish((k - 1, 1 - upper))

        @pl.when(k == STEPS - 1)
        def _():
            taken(far, k, 1 - upper)

        @pl.when(k > 0)
        def _():
            finish_other([(k - 1, 1 - upper)])

        taken(near, k, 0)
        finish((k, upper))

        @pl.when(k == STEPS - 1)
        def _():
            finish((k, 1 - upper))

        finish_other([(k, upper)])
        return carry

    def arrive_inner(k, carry):
        taken(near, k, 0)

        @pl.when(k < STEPS - 2)
        def _():
            taken(far, k + 1, 1 - upper, (3, outward))

        @pl.when(k == STEPS - 2)
        def _():
            taken(far, k + 1, 1 - upper, (3, outward), arrays=(1,))
            taken(far, k + 1, 1 - upper, arrays=(0,))

        @pl.when(k == STEPS - 1)
        def _():
            finish_other(finish((k, 0)))
            taken(near, k, 1)
            finish_other(finish((k, 1)))

        @pl.when(k < STEPS - 1)
        def _():
            taken(near, k, 1)
            done = finish((k, 0), (k, 1))

            @pl.when(k < STEPS - 2)
            def _():
                taken(far, k + 2, upper, (2, inward), (3, outward))

            finish_other(done)

        return carry

    @pl.when(is_end)
    def _():
        lax.fori_loop(0, STEPS, arrive_end, 0)
        finish_other([(STEPS - 1, 1 - upper)])

    @pl.when(is_inner)
    def _():
        taken(far, 0, upper, (2, inward), (3, outward))
        taken(far, 1, upper, (2, inward), (3, outward))
        taken(far, 0, 1 - upper, (3, outward))
        lax.fori_loop(0, STEPS, arrive_inner, 0)

    for copy in c_sends:
        copy.wait_recv()

    for p in range(n_ep):
        part = pl.ds(p * cap, cap)
        weight = jnp.broadcast_to(c_in[p], (LANES, capp)).T[:cap, :1]
        gate, up, grad = acc_g[part, :], acc_u[part, :], acc_h[part, :]
        sig = jax.nn.sigmoid(gate)
        silu = gate * sig
        hidden = silu * up
        score = jnp.sum(grad * hidden.astype(BF16).astype(F32), axis=1, keepdims=True)
        square[:cap, :] = jnp.broadcast_to(score, (cap, LANES))
        sc_in[tp, p] = square[...].T[:1, :]
        weighted = weight * grad
        hid[part, :] = (weight * hidden).astype(BF16)
        ggu[part, :units] = (weighted * up * sig * (1.0 + gate * (1.0 - sig))).astype(BF16)
        ggu[part, units:] = (weighted * silu).astype(BF16)

    def partial(share, offset=0, size=width):
        part = pl.ds(pl.multiple_of(share * width + offset, size), size)
        return dot_nt(ggu[:, :units], wg[part, :]) + dot_nt(ggu[:, units:], wu[part, :])

    sc_sends = []
    for k in range(1, n_tp):
        copy = remote(
            sc_in.at[tp], sc_in.at[tp], sc_s.at[k - 1], sc_r.at[k - 1],
            ep, lax.rem(tp + k, n_tp),
        )
        copy.start()
        sc_sends.append(copy)

    pairs, pair = nz // 2, z // 2
    owners = []
    for m in range(1, pairs):
        them = peer_of(pair, m, pairs)
        odd = lax.rem(them, 2)
        owners += [(m, 2 * them + odd), (m, 2 * them + 1 - odd)]
    n_far = 2 * len(owners)
    side, own = n_far, n_far + 1
    order = [q for _, q in owners[:1]] + [2 * pair + 1 - lax.rem(z, 2)]
    order += [q for _, q in owners[1:]] + [z]
    split = width // 2
    halves, moves = {}, {}

    def give_half(i):
        first[i] = partial(2 * order[i] + 1 - core).astype(BF16)
        halves[i] = remote(first.at[i], first_in.at[i], s1.at[i], r1.at[i], ep, sibling)
        halves[i].start()

    def spread(n):
        for d in far + near:
            p = peer_of(ep, d, n_ep)
            copy = remote(
                second.at[n, p], second_in.at[n, ep], s2.at[n, d - 1], r2.at[n, d - 1], p, tp
            )
            copy.start()
            moves[n, d] = copy

    crossing = remote(across_v, across_in, sa, ra, ep, across)

    def join(i):
        total = partial(2 * order[i] + core)
        halves[i].wait_recv()
        total = total + first_in[i].astype(F32)
        low, high = total[:, :split], total[:, split:].astype(BF16).reshape(second.shape[1:])
        if i == 1:
            across_v[...] = low.astype(BF16)
            crossing.start()
            second[side] = high
        elif i < nz - 1:
            n = 2 * max(i - 1, 0)
            second[n] = low.astype(BF16).reshape(second.shape[1:])
            spread(n)
            second[n + 1] = high
            spread(n + 1)
        else:
            own_total[...] = low
            second[own + 1] = high
            spread(side)
            spread(own + 1)

    def lead_part(h):
        return pl.ds(h * split, split)

    for h in range(2):
        first[0, :, lead_part(h)] = partial(
            2 * order[0] + 1 - core, h * split, split
        ).astype(BF16)
        halves[0, h] = remote(
            first.at[0, :, lead_part(h)], first_in.at[0, :, lead_part(h)],
            s1.at[h * nz], r1.at[h * nz], ep, sibling,
        )
        halves[0, h].start()
    for h in range(2):
        total = partial(2 * order[0] + core, h * split, split)
        halves[0, h].wait_recv()
        total = total + first_in[0, :, lead_part(h)].astype(F32)
        second[h] = total.astype(BF16).reshape(second.shape[1:])
        spread(h)
    give_half(1)
    for i in range(1, nz):
        if i < nz - 1:
            give_half(i + 1)
        join(i)

    def tile(t):
        return pl.ds(pl.multiple_of(t * width, width), width)

    def gate_up_step(t, carry):
        both = lax.dot_general(
            rows_v[0, :, :, tile(t)].reshape(rows, width), ggu[...],
            (((0,), (0,)), ((), ())), preferred_element_type=F32,
        ).astype(BF16)
        gate_out[tile(t), :] = both[:, :units]
        up_out[tile(t), :] = both[:, units:]
        return carry

    hidden_t = hid[...].T

    def down_step(t, carry):
        down_out[:, tile(t)] = jnp.dot(
            hidden_t, rows_v[1, :, :, tile(t)].reshape(rows, width),
            preferred_element_type=F32,
        ).astype(BF16)
        return carry

    def gather_tokens(n):
        for d in range(1, n_ep):
            moves[n, d].wait_recv()
        second_in[n, ep] = second[n, ep]
        return jnp.dot(
            pick[...], second_in[n].reshape(rows, split), preferred_element_type=F32
        )

    def to_collector(n):
        return remote(third.at[n], third_in.at[n], s3.at[n], r3.at[n], ep, across)

    def to_owner(n):
        m, q = owners[n // 2]
        slot = 2 * (m - 1) + n % 2
        return remote(
            third.at[n], final_in.at[slot], s4.at[n], r4.at[slot], ep, 2 * q + core
        )

    def gather_far(n):
        summed = gather_tokens(n)

        @pl.when(is_end)
        def _():
            third[n] = summed.astype(BF16)
            to_collector(n).start()

        @pl.when(is_inner)
        def _():
            held[n] = summed

    def collect(n):
        @pl.when(is_inner)
        def _():
            to_collector(n).wait_recv()
            third[n] = (held[n] + third_in[n].astype(F32)).astype(BF16)
            to_owner(n).start()

    def gate_up(part):
        lax.fori_loop(part * n_tp // 2, (part + 1) * n_tp // 2, gate_up_step, 0)

    def share_scores():
        for copy in sc_sends:
            copy.wait_recv()
        summed = sc_in[0]
        for t in range(1, n_tp):
            summed = summed + sc_in[t]
        tot[...] = summed
        for d in range(1, n_ep):
            p = peer_of(ep, d, n_ep)
            copy = remote(tot.at[p], tot_in.at[ep], tot_s.at[d - 1], tot_r.at[d - 1], p, tp)
            copy.start()
            tot_sends.append(copy)
        tot_in[ep] = tot[ep]

    def cross():
        crossing.wait_recv()
        total = own_total[...] + across_in[...].astype(F32)
        second[own] = total.astype(BF16).reshape(second.shape[1:])
        spread(own)

    def down(part):
        lax.fori_loop(part * n_tp // 2, (part + 1) * n_tp // 2, down_step, 0)

    tot_sends = []
    work = [
        lambda: gate_up(0), lambda: gate_up(1), share_scores, cross,
        lambda: down(0), lambda: down(1),
    ]
    for n in range(n_far):
        gather_far(n)
        for job in work[2 * n : 2 * n + 2]:
            job()
        if n:
            collect(n - 1)
    side_copy = remote(
        third.at[side], final_in.at[2 * (pairs - 1)],
        s4.at[side], r4.at[2 * (pairs - 1)], ep, across,
    )
    third[side] = gather_tokens(side).astype(BF16)
    side_copy.start()
    collect(n_far - 1)
    for copy in tot_sends:
        copy.wait_recv()
    score_r = [jnp.zeros((1, tokens), F32) for _ in range(top)]
    for e in range(n_ep):
        column = jnp.broadcast_to(tot_in[e], (LANES, capp)).T[:cap, :1]
        index = (lax.broadcasted_iota(jnp.int32, (cap, tokens), 0) + e * cap).astype(F32)
        for k in range(top):
            score_r[k] = score_r[k] + jnp.sum(
                jnp.where(index == tab[k : k + 1, :], column, 0.0), axis=0, keepdims=True
            )
    group = jnp.zeros((1, tokens), F32)
    for k in range(top):
        inner_out[k : k + 1, :] = gates[...] * score_r[k]
        group = group + inner[k : k + 1, :] * score_r[k]
    group_out[...] = group

    def final_copy(slot):
        return remote(
            third.at[0], final_in.at[slot], s4.at[0], r4.at[slot], ep, across
        )

    high = gather_tokens(own + 1)
    side_copy.wait_recv()
    high = high + final_in[2 * (pairs - 1)].astype(F32)
    for m in range(pairs - 1):
        final_copy(2 * m + 1).wait_recv()
        high = high + final_in[2 * m + 1].astype(F32)
    out[:, split:] = high.astype(BF16)
    low = gather_tokens(own)
    for m in range(pairs - 1):
        final_copy(2 * m).wait_recv()
        low = low + final_in[2 * m].astype(F32)
    out[:, :split] = low.astype(BF16)

    def drained(ref, slot):
        remote(ref, ref, drain.at[slot], drain.at[slot], ep, sibling).wait_send()

    @pl.when(is_end)
    def _():
        drained(sends.at[:, : len(near)], 0)
        if far:
            drained(sends.at[0, : len(far), :, :chunk], 1)
        drained(rows_v.at[0, : len(near), :, : half - chunk], 2)

    @pl.when(is_inner)
    def _():
        drained(sends.at[:, : n_ep - 1, :, : half // 2], 0)
        drained(sends.at[0, : len(near), :, :chunk], 1)
        if far:
            drained(rows_v.at[:, : len(far), :, : half // 2], 2)
            drained(rows_v.at[0, : len(far), :, : model - chunk], 3)

    drained(rows_v.at[:, : n_ep - 1, :, :half], 4)
    for copy in c_sends + sc_sends + tot_sends + list(halves.values()) + list(moves.values()):
        copy.wait_send()
    crossing.wait_send()
    side_copy.wait_send()

    @pl.when(is_end)
    def _():
        for n in range(n_far):
            to_collector(n).wait_send()

    @pl.when(is_inner)
    def _():
        for n in range(n_far):
            to_owner(n).wait_send()


def layer(n_ep, n_tp, cap, route, gates, inner, tokens, cotangent, wg, wu, wd):
    vmem = pl.BlockSpec(memory_space=pltpu.VMEM)
    any_spec = pl.BlockSpec(memory_space=pl.ANY)
    nz = n_tp // 2
    count, model = tokens.shape
    rows, units = n_ep * cap, wg.shape[1]
    width, half = model // n_tp, model // 2
    capp = -(-cap // LANES) * LANES
    dma = pltpu.SemaphoreType.DMA
    return pl.pallas_call(
        functools.partial(layer_kernel, n_ep, n_tp, cap),
        out_shape=(
            pltpu.VMEM((count, width), BF16),
            pltpu.VMEM(gates.shape, F32),
            pltpu.VMEM(inner.shape, F32),
            pltpu.VMEM(wg.shape, BF16),
            pltpu.VMEM(wu.shape, BF16),
            pltpu.VMEM(wd.shape, BF16),
        ),
        in_specs=[vmem] * 3 + [any_spec] * 5,
        out_specs=(vmem,) * 6,
        scratch_shapes=[
            pltpu.VMEM((2, count, model), BF16),
            pltpu.VMEM((2, n_ep, cap, half), BF16),
            pltpu.VMEM((2, n_ep, cap, model), BF16),
            pltpu.VMEM(wg.shape, BF16),
            pltpu.VMEM(wu.shape, BF16),
            pltpu.VMEM(wd.shape, BF16),
            pltpu.VMEM((8, count), F32),
            pltpu.VMEM((rows, count), BF16),
            pltpu.VMEM((count, rows), BF16),
            pltpu.VMEM((n_ep, 1, capp), F32),
            pltpu.VMEM((n_ep, 1, capp), F32),
            pltpu.VMEM((capp, LANES), F32),
            pltpu.VMEM((n_tp, n_ep, 1, capp), F32),
            pltpu.VMEM((n_ep, 1, capp), F32),
            pltpu.VMEM((n_ep, 1, capp), F32),
            pltpu.VMEM((rows, units), F32),
            pltpu.VMEM((rows, units), F32),
            pltpu.VMEM((rows, units), F32),
            pltpu.VMEM((rows, 2 * units), BF16),
            pltpu.VMEM((rows, units), BF16),
            pltpu.VMEM((nz, rows, width), BF16),
            pltpu.VMEM((nz, rows, width), BF16),
            pltpu.VMEM((2 * nz - 1, n_ep, cap, width // 2), BF16),
            pltpu.VMEM((2 * nz - 1, n_ep, cap, width // 2), BF16),
            pltpu.VMEM((rows, width // 2), BF16),
            pltpu.VMEM((rows, width // 2), BF16),
            pltpu.VMEM((rows, width // 2), F32),
            pltpu.VMEM((2 * nz - 3, count, width // 2), BF16),
            pltpu.VMEM((2 * nz - 4, count, width // 2), BF16),
            pltpu.VMEM((2 * nz - 4, count, width // 2), F32),
            pltpu.VMEM((nz - 1, count, width // 2), BF16),
            dma((7,)),
            dma((5,)),
            dma((2, n_ep - 1, STEPS, 2)),
            dma((2, n_ep - 1, STEPS, 2)),
            dma((n_ep - 1,)), dma((n_ep - 1,)),
            dma((n_tp - 1,)), dma((n_tp - 1,)),
            dma((n_ep - 1,)), dma((n_ep - 1,)),
            dma((nz + 1,)), dma((nz + 1,)),
            dma((2 * nz - 1, n_ep - 1)), dma((2 * nz - 1, n_ep - 1)),
            dma((2 * nz - 4,)), dma((2 * nz - 4,)),
            dma((2 * nz - 3,)), dma((nz - 1,)),
            dma, dma,
        ],
        compiler_params=pltpu.CompilerParams(
            collective_id=0, has_side_effects=True, vmem_limit_bytes=54 * 1024 * 1024
        ),
    )(route, gates, inner, tokens, cotangent, wg, wu, wd)


def deliver_kernel(count, *refs):
    sems = refs[-1]
    copies = [
        pltpu.make_async_copy(refs[i], refs[count + i], sems.at[i]) for i in range(count)
    ]
    for copy in copies:
        copy.start()
    for copy in copies:
        copy.wait()


def deliver(*arrays):
    count = len(arrays)
    return pl.pallas_call(
        functools.partial(deliver_kernel, count),
        out_shape=tuple(jax.ShapeDtypeStruct(a.shape, a.dtype) for a in arrays),
        in_specs=[pl.BlockSpec(memory_space=pltpu.VMEM)] * count,
        out_specs=(pl.BlockSpec(memory_space=pl.ANY),) * count,
        scratch_shapes=[pltpu.SemaphoreType.DMA((count,))],
        compiler_params=pltpu.CompilerParams(vmem_limit_bytes=4 * 1024 * 1024),
    )(*arrays)


def per_device(tokens, cotangent, routing, group_gate, inner_gate, w_gate, w_up, w_down):
    n_ep, n_tp = lax.axis_size("ep"), lax.axis_size("tp")
    cap = tokens.shape[0] * routing.shape[1] * 5 // (4 * n_ep)
    results = layer(
        n_ep, n_tp, cap, routing.T, group_gate[None], inner_gate.T,
        tokens, cotangent, w_gate[0], w_up[0], w_down[0],
    )
    token_grad, group_grad, inner_grad, gate_grad, upper_grad, down_grad = deliver(*[
        pltpu.with_memory_space_constraint(r, pltpu.VMEM) for r in results
    ])
    return (
        token_grad,
        group_grad[0],
        inner_grad.T,
        gate_grad[None],
        upper_grad[None],
        down_grad[None],
    )


def solution(mesh):
    return jax.shard_map(
        per_device,
        mesh=mesh,
        in_specs=(
            P("ep", None),
            P("ep", None),
            P("ep", None),
            P("ep"),
            P("ep", None),
            P("ep", None, "tp"),
            P("ep", None, "tp"),
            P("ep", "tp", None),
        ),
        out_specs=(
            P("ep", "tp"),
            P("ep"),
            P("ep", None),
            P("ep", None, "tp"),
            P("ep", None, "tp"),
            P("ep", "tp", None),
        ),
        check_vma=False,
    )
```

```python
import functools

import jax
import jax.numpy as jnp
from jax import lax
from jax.experimental import pallas as pl
from jax.experimental.pallas import tpu as pltpu
from jax.sharding import PartitionSpec as P

LANES = 128
STEPS = 4
BF16 = jnp.bfloat16
F32 = jnp.float32


def peer_of(me, d, n):
    if n & (n - 1):
        return lax.rem(2 * n + d - me, n)
    out, bit = me, 1
    while bit < n:
        if d & bit:
            out = out + bit * (1 - 2 * lax.rem(me // bit, 2))
        bit *= 2
    return out


def barrier(partners):
    sem = pltpu.get_barrier_semaphore()
    for ep, tp in partners:
        pl.semaphore_signal(
            sem, inc=1, device_id=(ep, tp), device_id_type=pl.DeviceIdType.MESH
        )
    return lambda: pl.semaphore_wait(sem, len(partners))


def remote(src, dst, send, recv, ep, tp):
    return pltpu.make_async_remote_copy(
        src_ref=src,
        dst_ref=dst,
        send_sem=send,
        recv_sem=recv,
        device_id=(ep, tp),
        device_id_type=pl.DeviceIdType.MESH,
    )


def dot_nt(a, b):
    return lax.dot_general(a, b, (((1,), (1,)), ((), ())), preferred_element_type=F32)


def layer_kernel(n_ep, n_tp, cap, route, gates, inner, tok_hbm, cot_hbm, wg_hbm, wu_hbm, wd_hbm,
                 out, group_out, inner_out, gate_out, up_out, down_out,
                 toks, sends, rows_v, wg, wu, wd, tab, put, pick,
                 cs, c_in, square, sc_in, tot, tot_in,
                 acc_g, acc_u, acc_h, ggu, hid,
                 first, first_in, second, second_in, across_v, across_in, own_total,
                 third, third_in, held, final_in,
                 local, drain, recv, sib_recv, c_s, c_r, sc_s, sc_r, tot_s, tot_r,
                 s1, r1, s2, r2, s3, r3, s4, r4, sa, ra):
    ep, tp = lax.axis_index("ep"), lax.axis_index("tp")
    core = lax.rem(tp, 2)
    z = tp // 2
    nz = n_tp // 2
    sibling = tp + 1 - 2 * core
    across = tp + 2 - 4 * lax.rem(z, 2)
    spot = lax.rem(z, 4)
    is_end = jnp.logical_or(spot == 0, spot == 3)
    is_inner = jnp.logical_not(is_end)
    upper = spot // 2
    inward = tp + 2 - 4 * upper
    outward = tp - 2 + 4 * upper
    tokens, model = toks.shape[1], toks.shape[2]
    top = route.shape[0]
    half = model // 2
    chunk = half // (2 * STEPS)
    base = core * half
    rows = n_ep * cap
    capp = cs.shape[2]
    units = wg.shape[1]
    width = out.shape[1]
    near = [d for d in range(1, n_ep) if not d & (d - 1)]
    far = [d for d in range(1, n_ep) if d & (d - 1)]
    everyone = [(peer_of(ep, d, n_ep), tp) for d in range(1, n_ep)]
    everyone += [(ep, lax.rem(tp + k, n_tp)) for k in range(1, n_tp)]

    def cols(start, size):
        return pl.ds(pl.multiple_of(start, LANES), size)

    loads = []
    for h in (core, 1 - core):
        for a, src in enumerate((tok_hbm, cot_hbm)):
            part = cols(h * half, half)
            loads.append(pltpu.make_async_copy(
                src.at[:, part], toks.at[a, :, part], local.at[len(loads)]
            ))
    for src, dst in ((wg_hbm, wg), (wu_hbm, wu), (wd_hbm, wd)):
        loads.append(pltpu.make_async_copy(src, dst, local.at[len(loads)]))
    for load in loads:
        load.start()
    entered = barrier(everyone)

    route_v = route[...]
    expert = lax.broadcasted_iota(jnp.int32, (-(-n_ep // 16) * 16, tokens), 0)
    names = jnp.zeros(expert.shape, F32)
    for k in range(top):
        names = names + jnp.where(route_v[k : k + 1] == expert, 1.0, 0.0)
    earlier = jnp.where(
        lax.broadcasted_iota(jnp.int32, (tokens, tokens), 0)
        < lax.broadcasted_iota(jnp.int32, (tokens, tokens), 1), 1.0, 0.0,
    ).astype(BF16)
    rank = jnp.dot(names.astype(BF16), earlier, preferred_element_type=F32)
    place_of = (expert * cap).astype(F32) + rank
    tab[...] = jnp.zeros_like(tab)
    slot_r = []
    for k in range(top):
        slot = jnp.sum(
            jnp.where(route_v[k : k + 1] == expert, place_of, 0.0), axis=0, keepdims=True
        )
        slot_r.append(slot)
        tab[k : k + 1, :] = slot
        tab[top + k : top + k + 1, :] = gates[...] * inner[k : k + 1, :]
    turned = tab[...].T
    slot_c = [turned[:, k : k + 1] for k in range(top)]
    comb_c = [turned[:, top + k : top + k + 1] for k in range(top)]

    def one_hot(index, slots):
        hit = index == slots[0]
        for slot in slots[1:]:
            hit = jnp.logical_or(hit, index == slot)
        return jnp.where(hit, 1.0, 0.0).astype(BF16)

    put[...] = one_hot(
        lax.broadcasted_iota(jnp.int32, (rows, tokens), 0).astype(F32), slot_r
    )
    own_put = one_hot(
        (lax.broadcasted_iota(jnp.int32, (cap, tokens), 0) + ep * cap).astype(F32), slot_r
    )

    def piece(a, p, k, side):
        return rows_v.at[a, p, :, cols(base + (k + STEPS * side) * chunk, chunk)]

    def direct(a, d, k, side, slot=0):
        p = peer_of(ep, d, n_ep)
        return remote(
            sends.at[a, p, :, cols((k + STEPS * side) * chunk, chunk)],
            piece(a, ep, k, side),
            drain.at[slot], recv.at[a, d - 1, k, side], p, tp,
        )

    def along(a, d, k, side, slot, target):
        p = peer_of(ep, d, n_ep)
        return remote(
            piece(a, p, k, side), piece(a, p, k, side),
            drain.at[slot], recv.at[a, d - 1, k, side], ep, target,
        )

    def to_sibling(a, d, k, side):
        p = peer_of(ep, d, n_ep)
        return remote(
            piece(a, p, k, side), piece(a, p, k, side),
            drain.at[4], sib_recv.at[a, d - 1, k, side], ep, sibling,
        )

    def place(k):
        for side in (1, 0):
            at = (k + STEPS * side) * chunk
            for a in range(2):
                placed = jnp.dot(
                    put[...], toks[a, :, cols(base + at, chunk)], preferred_element_type=F32
                ).astype(BF16).reshape(n_ep, cap, chunk)
                sends[a, :, :, cols(at, chunk)] = placed
                rows_v[a, ep, :, cols(base + at, chunk)] = sends[a, ep, :, cols(at, chunk)]

    def send_out(k):
        @pl.when(is_end)
        def _():
            for a in range(2):
                for d in near:
                    direct(a, d, k, 1).start()

            @pl.when(k == STEPS - 1)
            def _():
                for d in far:
                    direct(0, d, k, 1 - upper, 1).start()

            for a in range(2):
                for d in near:
                    direct(a, d, k, 0).start()

        @pl.when(is_inner)
        def _():
            for a in range(2):
                for d in far:
                    direct(a, d, k, upper).start()

            @pl.when(k > 0)
            def _():
                for a in range(2):
                    for d in near:
                        direct(a, d, k - 1, 0).start()

            @pl.when(k == STEPS - 1)
            def _():
                for a in range(2):
                    for d in near:
                        direct(a, d, k, 0).start()
                for d in near:
                    direct(0, d, k, 1, 1).start()

    loads[0].wait()
    loads[1].wait()
    place(0)
    entered()
    send_out(0)

    def place_step(k, carry):
        place(k)
        send_out(k)
        return carry

    lax.fori_loop(1, STEPS, place_step, 0)

    lane = lax.broadcasted_iota(jnp.int32, (tokens, capp), 1)
    lane_f = lane.astype(F32)
    for e in range(n_ep):
        weight = jnp.zeros((tokens, capp), F32)
        for k in range(top):
            hit = jnp.logical_and(lane_f == slot_c[k] - float(e * cap), lane < cap)
            weight = weight + jnp.where(hit, comb_c[k], 0.0)
        cs[e] = jnp.sum(weight, axis=0, keepdims=True)
    c_sends = []
    for d in range(1, n_ep):
        p = peer_of(ep, d, n_ep)
        copy = remote(cs.at[p], c_in.at[ep], c_s.at[d - 1], c_r.at[d - 1], p, tp)
        copy.start()
        c_sends.append(copy)
    c_in[ep] = cs[ep]
    pick[...] = one_hot(
        lax.broadcasted_iota(jnp.int32, (tokens, rows), 1).astype(F32), slot_c
    )
    square[...] = jnp.zeros_like(square)
    acc_g[...] = jnp.zeros_like(acc_g)
    acc_u[...] = jnp.zeros_like(acc_u)
    acc_h[...] = jnp.zeros_like(acc_h)
    loads[2].wait()
    loads[3].wait()
    other = (1 - core) * half
    for a in range(2):
        def own_step(j, carry, a=a):
            part = cols(other + j * (half // 4), half // 4)
            rows_v[a, ep, :, part] = jnp.dot(
                own_put, toks[a, :, part], preferred_element_type=F32
            ).astype(BF16)
            return carry

        lax.fori_loop(0, 4, own_step, 0)
    for load in loads[4:]:
        load.wait()

    def accumulate(h, k, side):
        part = cols(h * half + (k + STEPS * side) * chunk, chunk)
        source = [rows_v[a, :, :, part].reshape(rows, chunk) for a in range(2)]
        for acc, w in ((acc_g, wg), (acc_u, wu)):
            acc[...] += jnp.dot(source[0], w[part, :], preferred_element_type=F32)
        acc_h[...] += dot_nt(source[1], wd[:, part])

    def taken(ds, k, side, *targets, arrays=(0, 1)):
        for a in arrays:
            for d in ds:
                direct(a, d, k, side).wait_recv()
                for slot, target in targets:
                    along(a, d, k, side, slot, target).start()
                to_sibling(a, d, k, side).start()

    def finish(*pieces):
        for k, side in pieces:
            accumulate(core, k, side)
        return pieces

    def finish_other(pieces):
        for k, side in pieces:
            for a in range(2):
                for d in range(1, n_ep):
                    to_sibling(a, d, k, side).wait_recv()
            accumulate(1 - core, k, side)

    def arrive_end(k, carry):
        @pl.when(k < STEPS - 1)
        def _():
            taken(near, k, 1, (2, inward))

        @pl.when(k == STEPS - 1)
        def _():
            taken(near, k, 1, (2, inward), arrays=(1,))
            taken(near, k, 1, arrays=(0,))

        @pl.when(k > 0)
        def _():
            taken(far, k - 1, 1 - upper)

        taken(far, k, upper)

        @pl.when(k > 0)
        def _():
            finish((k - 1, 1 - upper))

        @pl.when(k == STEPS - 1)
        def _():
            taken(far, k, 1 - upper)

        @pl.when(k > 0)
        def _():
            finish_other([(k - 1, 1 - upper)])

        taken(near, k, 0)
        finish((k, upper))

        @pl.when(k == STEPS - 1)
        def _():
            finish((k, 1 - upper))

        finish_other([(k, upper)])
        return carry

    def arrive_inner(k, carry):
        taken(near, k, 0)

        @pl.when(k < STEPS - 2)
        def _():
            taken(far, k + 1, 1 - upper, (3, outward))

        @pl.when(k == STEPS - 2)
        def _():
            taken(far, k + 1, 1 - upper, (3, outward), arrays=(1,))
            taken(far, k + 1, 1 - upper, arrays=(0,))

        @pl.when(k == STEPS - 1)
        def _():
            finish_other(finish((k, 0)))
            taken(near, k, 1)
            finish_other(finish((k, 1)))

        @pl.when(k < STEPS - 1)
        def _():
            taken(near, k, 1)
            done = finish((k, 0), (k, 1))

            @pl.when(k < STEPS - 2)
            def _():
                taken(far, k + 2, upper, (2, inward), (3, outward))

            finish_other(done)

        return carry

    @pl.when(is_end)
    def _():
        lax.fori_loop(0, STEPS, arrive_end, 0)
        finish_other([(STEPS - 1, 1 - upper)])

    @pl.when(is_inner)
    def _():
        taken(far, 0, upper, (2, inward), (3, outward))
        taken(far, 1, upper, (2, inward), (3, outward))
        taken(far, 0, 1 - upper, (3, outward))
        lax.fori_loop(0, STEPS, arrive_inner, 0)

    for copy in c_sends:
        copy.wait_recv()

    def partial(share, offset=0, size=width, own=slice(None)):
        part = pl.ds(pl.multiple_of(share * width + offset, size), size)
        return dot_nt(ggu[own, :units], wg[part, :]) + dot_nt(ggu[own, units:], wu[part, :])

    pairs, pair = nz // 2, z // 2
    owners = []
    for m in range(1, pairs):
        them = peer_of(pair, m, pairs)
        odd = lax.rem(them, 2)
        owners += [(m, 2 * them + odd), (m, 2 * them + 1 - odd)]
    n_far = 2 * len(owners)
    side, own = n_far, n_far + 1
    order = [q for _, q in owners[:1]] + [2 * pair + 1 - lax.rem(z, 2)]
    order += [q for _, q in owners[1:]] + [z]
    split = width // 2

    for p in range(n_ep):
        part = pl.ds(p * cap, cap)
        weight = jnp.broadcast_to(c_in[p], (LANES, capp)).T[:cap, :1]
        gate, up, grad = acc_g[part, :], acc_u[part, :], acc_h[part, :]
        sig = jax.nn.sigmoid(gate)
        silu = gate * sig
        hidden = silu * up
        score = jnp.sum(grad * hidden.astype(BF16).astype(F32), axis=1, keepdims=True)
        square[:cap, :] = jnp.broadcast_to(score, (cap, LANES))
        sc_in[tp, p] = square[...].T[:1, :]
        weighted = weight * grad
        hid[part, :] = (weight * hidden).astype(BF16)
        ggu[part, :units] = (weighted * up * sig * (1.0 + gate * (1.0 - sig))).astype(BF16)
        ggu[part, units:] = (weighted * silu).astype(BF16)
        first[0, part, :] = partial(2 * order[0] + 1 - core, own=part).astype(BF16)

    sc_sends = []
    for k in range(1, n_tp):
        copy = remote(
            sc_in.at[tp], sc_in.at[tp], sc_s.at[k - 1], sc_r.at[k - 1],
            ep, lax.rem(tp + k, n_tp),
        )
        copy.start()
        sc_sends.append(copy)

    halves, moves = {}, {}

    def give_half(i):
        first[i] = partial(2 * order[i] + 1 - core).astype(BF16)
        halves[i] = remote(first.at[i], first_in.at[i], s1.at[i], r1.at[i], ep, sibling)
        halves[i].start()

    def spread(n):
        for d in far + near:
            p = peer_of(ep, d, n_ep)
            copy = remote(
                second.at[n, p], second_in.at[n, ep], s2.at[n, d - 1], r2.at[n, d - 1], p, tp
            )
            copy.start()
            moves[n, d] = copy

    crossing = remote(across_v, across_in, sa, ra, ep, across)

    def join(i):
        total = partial(2 * order[i] + core)
        halves[i].wait_recv()
        total = total + first_in[i].astype(F32)
        low, high = total[:, :split], total[:, split:].astype(BF16).reshape(second.shape[1:])
        if i == 1:
            across_v[...] = low.astype(BF16)
            crossing.start()
            second[side] = high
        elif i < nz - 1:
            n = 2 * max(i - 1, 0)
            second[n] = low.astype(BF16).reshape(second.shape[1:])
            spread(n)
            second[n + 1] = high
            spread(n + 1)
        else:
            own_total[...] = low
            second[own + 1] = high
            spread(side)
            spread(own + 1)

    def lead_part(h):
        return pl.ds(h * split, split)

    for h in range(2):
        halves[0, h] = remote(
            first.at[0, :, lead_part(h)], first_in.at[0, :, lead_part(h)],
            s1.at[h * nz], r1.at[h * nz], ep, sibling,
        )
        halves[0, h].start()
    for h in range(2):
        total = partial(2 * order[0] + core, h * split, split)
        halves[0, h].wait_recv()
        total = total + first_in[0, :, lead_part(h)].astype(F32)
        second[h] = total.astype(BF16).reshape(second.shape[1:])
        spread(h)
    give_half(1)
    for i in range(1, nz):
        if i < nz - 1:
            give_half(i + 1)
        join(i)

    def tile(t):
        return pl.ds(pl.multiple_of(t * width, width), width)

    def gate_up_step(t, carry):
        both = lax.dot_general(
            rows_v[0, :, :, tile(t)].reshape(rows, width), ggu[...],
            (((0,), (0,)), ((), ())), preferred_element_type=F32,
        ).astype(BF16)
        gate_out[tile(t), :] = both[:, :units]
        up_out[tile(t), :] = both[:, units:]
        return carry

    hidden_t = hid[...].T

    def down_step(t, carry):
        down_out[:, tile(t)] = jnp.dot(
            hidden_t, rows_v[1, :, :, tile(t)].reshape(rows, width),
            preferred_element_type=F32,
        ).astype(BF16)
        return carry

    def gather_tokens(n):
        for d in range(1, n_ep):
            moves[n, d].wait_recv()
        second_in[n, ep] = second[n, ep]
        return jnp.dot(
            pick[...], second_in[n].reshape(rows, split), preferred_element_type=F32
        )

    def to_collector(n):
        return remote(third.at[n], third_in.at[n], s3.at[n], r3.at[n], ep, across)

    def to_owner(n):
        m, q = owners[n // 2]
        slot = 2 * (m - 1) + n % 2
        return remote(
            third.at[n], final_in.at[slot], s4.at[n], r4.at[slot], ep, 2 * q + core
        )

    def gather_far(n):
        summed = gather_tokens(n)

        @pl.when(is_end)
        def _():
            third[n] = summed.astype(BF16)
            to_collector(n).start()

        @pl.when(is_inner)
        def _():
            held[n] = summed

    def collect(n):
        @pl.when(is_inner)
        def _():
            to_collector(n).wait_recv()
            third[n] = (held[n] + third_in[n].astype(F32)).astype(BF16)
            to_owner(n).start()

    def gate_up(part):
        lax.fori_loop(part * n_tp // 2, (part + 1) * n_tp // 2, gate_up_step, 0)

    def share_scores():
        for copy in sc_sends:
            copy.wait_recv()
        summed = sc_in[0]
        for t in range(1, n_tp):
            summed = summed + sc_in[t]
        tot[...] = summed
        for d in range(1, n_ep):
            p = peer_of(ep, d, n_ep)
            copy = remote(tot.at[p], tot_in.at[ep], tot_s.at[d - 1], tot_r.at[d - 1], p, tp)
            copy.start()
            tot_sends.append(copy)
        tot_in[ep] = tot[ep]

    def cross():
        crossing.wait_recv()
        total = own_total[...] + across_in[...].astype(F32)
        second[own] = total.astype(BF16).reshape(second.shape[1:])
        spread(own)

    def down(part):
        lax.fori_loop(part * n_tp // 2, (part + 1) * n_tp // 2, down_step, 0)

    tot_sends = []
    work = [
        lambda: gate_up(0), lambda: gate_up(1), share_scores, cross,
        lambda: down(0), lambda: down(1),
    ]
    for n in range(n_far):
        gather_far(n)
        for job in work[2 * n : 2 * n + 2]:
            job()
        if n:
            collect(n - 1)
    side_copy = remote(
        third.at[side], final_in.at[2 * (pairs - 1)],
        s4.at[side], r4.at[2 * (pairs - 1)], ep, across,
    )
    third[side] = gather_tokens(side).astype(BF16)
    side_copy.start()
    collect(n_far - 1)
    for copy in tot_sends:
        copy.wait_recv()
    score_r = [jnp.zeros((1, tokens), F32) for _ in range(top)]
    for e in range(n_ep):
        column = jnp.broadcast_to(tot_in[e], (LANES, capp)).T[:cap, :1]
        index = (lax.broadcasted_iota(jnp.int32, (cap, tokens), 0) + e * cap).astype(F32)
        for k in range(top):
            score_r[k] = score_r[k] + jnp.sum(
                jnp.where(index == tab[k : k + 1, :], column, 0.0), axis=0, keepdims=True
            )
    group = jnp.zeros((1, tokens), F32)
    for k in range(top):
        inner_out[k : k + 1, :] = gates[...] * score_r[k]
        group = group + inner[k : k + 1, :] * score_r[k]
    group_out[...] = group

    def final_copy(slot):
        return remote(
            third.at[0], final_in.at[slot], s4.at[0], r4.at[slot], ep, across
        )

    high = gather_tokens(own + 1)
    side_copy.wait_recv()
    high = high + final_in[2 * (pairs - 1)].astype(F32)
    for m in range(pairs - 1):
        final_copy(2 * m + 1).wait_recv()
        high = high + final_in[2 * m + 1].astype(F32)
    out[:, split:] = high.astype(BF16)
    low = gather_tokens(own)
    for m in range(pairs - 1):
        final_copy(2 * m).wait_recv()
        low = low + final_in[2 * m].astype(F32)
    out[:, :split] = low.astype(BF16)

    def drained(ref, slot):
        remote(ref, ref, drain.at[slot], drain.at[slot], ep, sibling).wait_send()

    @pl.when(is_end)
    def _():
        drained(sends.at[:, : len(near)], 0)
        if far:
            drained(sends.at[0, : len(far), :, :chunk], 1)
        drained(rows_v.at[0, : len(near), :, : half - chunk], 2)

    @pl.when(is_inner)
    def _():
        drained(sends.at[:, : n_ep - 1, :, : half // 2], 0)
        drained(sends.at[0, : len(near), :, :chunk], 1)
        if far:
            drained(rows_v.at[:, : len(far), :, : half // 2], 2)
            drained(rows_v.at[0, : len(far), :, : model - chunk], 3)

    drained(rows_v.at[:, : n_ep - 1, :, :half], 4)
    for copy in c_sends + sc_sends + tot_sends + list(halves.values()) + list(moves.values()):
        copy.wait_send()
    crossing.wait_send()
    side_copy.wait_send()

    @pl.when(is_end)
    def _():
        for n in range(n_far):
            to_collector(n).wait_send()

    @pl.when(is_inner)
    def _():
        for n in range(n_far):
            to_owner(n).wait_send()


def layer(n_ep, n_tp, cap, route, gates, inner, tokens, cotangent, wg, wu, wd):
    vmem = pl.BlockSpec(memory_space=pltpu.VMEM)
    any_spec = pl.BlockSpec(memory_space=pl.ANY)
    nz = n_tp // 2
    count, model = tokens.shape
    rows, units = n_ep * cap, wg.shape[1]
    width, half = model // n_tp, model // 2
    capp = -(-cap // LANES) * LANES
    dma = pltpu.SemaphoreType.DMA
    return pl.pallas_call(
        functools.partial(layer_kernel, n_ep, n_tp, cap),
        out_shape=(
            pltpu.VMEM((count, width), BF16),
            pltpu.VMEM(gates.shape, F32),
            pltpu.VMEM(inner.shape, F32),
            pltpu.VMEM(wg.shape, BF16),
            pltpu.VMEM(wu.shape, BF16),
            pltpu.VMEM(wd.shape, BF16),
        ),
        in_specs=[vmem] * 3 + [any_spec] * 5,
        out_specs=(vmem,) * 6,
        scratch_shapes=[
            pltpu.VMEM((2, count, model), BF16),
            pltpu.VMEM((2, n_ep, cap, half), BF16),
            pltpu.VMEM((2, n_ep, cap, model), BF16),
            pltpu.VMEM(wg.shape, BF16),
            pltpu.VMEM(wu.shape, BF16),
            pltpu.VMEM(wd.shape, BF16),
            pltpu.VMEM((8, count), F32),
            pltpu.VMEM((rows, count), BF16),
            pltpu.VMEM((count, rows), BF16),
            pltpu.VMEM((n_ep, 1, capp), F32),
            pltpu.VMEM((n_ep, 1, capp), F32),
            pltpu.VMEM((capp, LANES), F32),
            pltpu.VMEM((n_tp, n_ep, 1, capp), F32),
            pltpu.VMEM((n_ep, 1, capp), F32),
            pltpu.VMEM((n_ep, 1, capp), F32),
            pltpu.VMEM((rows, units), F32),
            pltpu.VMEM((rows, units), F32),
            pltpu.VMEM((rows, units), F32),
            pltpu.VMEM((rows, 2 * units), BF16),
            pltpu.VMEM((rows, units), BF16),
            pltpu.VMEM((nz, rows, width), BF16),
            pltpu.VMEM((nz, rows, width), BF16),
            pltpu.VMEM((2 * nz - 1, n_ep, cap, width // 2), BF16),
            pltpu.VMEM((2 * nz - 1, n_ep, cap, width // 2), BF16),
            pltpu.VMEM((rows, width // 2), BF16),
            pltpu.VMEM((rows, width // 2), BF16),
            pltpu.VMEM((rows, width // 2), F32),
            pltpu.VMEM((2 * nz - 3, count, width // 2), BF16),
            pltpu.VMEM((2 * nz - 4, count, width // 2), BF16),
            pltpu.VMEM((2 * nz - 4, count, width // 2), F32),
            pltpu.VMEM((nz - 1, count, width // 2), BF16),
            dma((7,)),
            dma((5,)),
            dma((2, n_ep - 1, STEPS, 2)),
            dma((2, n_ep - 1, STEPS, 2)),
            dma((n_ep - 1,)), dma((n_ep - 1,)),
            dma((n_tp - 1,)), dma((n_tp - 1,)),
            dma((n_ep - 1,)), dma((n_ep - 1,)),
            dma((nz + 1,)), dma((nz + 1,)),
            dma((2 * nz - 1, n_ep - 1)), dma((2 * nz - 1, n_ep - 1)),
            dma((2 * nz - 4,)), dma((2 * nz - 4,)),
            dma((2 * nz - 3,)), dma((nz - 1,)),
            dma, dma,
        ],
        compiler_params=pltpu.CompilerParams(
            collective_id=0, has_side_effects=True, vmem_limit_bytes=54 * 1024 * 1024
        ),
    )(route, gates, inner, tokens, cotangent, wg, wu, wd)


def deliver_kernel(count, *refs):
    sems = refs[-1]
    copies = [
        pltpu.make_async_copy(refs[i], refs[count + i], sems.at[i]) for i in range(count)
    ]
    for copy in copies:
        copy.start()
    for copy in copies:
        copy.wait()


def deliver(*arrays):
    count = len(arrays)
    return pl.pallas_call(
        functools.partial(deliver_kernel, count),
        out_shape=tuple(jax.ShapeDtypeStruct(a.shape, a.dtype) for a in arrays),
        in_specs=[pl.BlockSpec(memory_space=pltpu.VMEM)] * count,
        out_specs=(pl.BlockSpec(memory_space=pl.ANY),) * count,
        scratch_shapes=[pltpu.SemaphoreType.DMA((count,))],
        compiler_params=pltpu.CompilerParams(vmem_limit_bytes=4 * 1024 * 1024),
    )(*arrays)


def per_device(tokens, cotangent, routing, group_gate, inner_gate, w_gate, w_up, w_down):
    n_ep, n_tp = lax.axis_size("ep"), lax.axis_size("tp")
    cap = tokens.shape[0] * routing.shape[1] * 5 // (4 * n_ep)
    results = layer(
        n_ep, n_tp, cap, routing.T, group_gate[None], inner_gate.T,
        tokens, cotangent, w_gate[0], w_up[0], w_down[0],
    )
    token_grad, group_grad, inner_grad, gate_grad, upper_grad, down_grad = deliver(*[
        pltpu.with_memory_space_constraint(r, pltpu.VMEM) for r in results
    ])
    return (
        token_grad,
        group_grad[0],
        inner_grad.T,
        gate_grad[None],
        upper_grad[None],
        down_grad[None],
    )


def solution(mesh):
    return jax.shard_map(
        per_device,
        mesh=mesh,
        in_specs=(
            P("ep", None),
            P("ep", None),
            P("ep", None),
            P("ep"),
            P("ep", None),
            P("ep", None, "tp"),
            P("ep", None, "tp"),
            P("ep", "tp", None),
        ),
        out_specs=(
            P("ep", "tp"),
            P("ep"),
            P("ep", None),
            P("ep", None, "tp"),
            P("ep", None, "tp"),
            P("ep", "tp", None),
        ),
        check_vma=False,
    )
```
